32 devices in a mesh: sp: 8 (over z, x), tp: 4 (over y, core).
Axes of the slice: x: 2, y: 2, z: 4, core: 2. Of those that a mesh axis runs over, the one named last changes fastest.
Arguments:
- tokens: bfloat16 [1536, 2048], P(('sp', 'tp')), may hold values from -7 to 7
- input_norm_gain: float32 [2048], replicated, may hold values from 0.1 to 1.9
- paired_query_weight: bfloat16 [2048, 512], P('sp', 'tp'), may hold values from -16 to 16
- shared_key_weight: bfloat16 [2048, 64], replicated, may hold values from -1 to 1
- shared_value_weight: bfloat16 [2048, 64], replicated, may hold values from -0.125 to 0.125
- recurrent_query_weight: bfloat16 [2048, 1024], P('sp', 'tp'), may hold values from -0.125 to 0.125
- forget_gate_weight: bfloat16 [2048, 1024], P('sp', 'tp'), may hold values from -0.125 to 0.125
- recurrent_value_weight: bfloat16 [2048, 1024], P('sp', 'tp'), may hold values from -0.125 to 0.125
- attention_output_weight: bfloat16 [2048, 512], P('sp', 'tp'), may hold values from -0.15625 to 0.15625
- recurrent_output_weight: bfloat16 [2048, 1024], P('sp', 'tp'), may hold values from -0.15625 to 0.15625
- attention_head_gain: float32 [64], replicated, may hold values from 0.1 to 1.9
- recurrent_head_gain: float32 [128], replicated, may hold values from 0.1 to 1.9
- second_map_weight: float32 [8], P('tp'), may hold values from 0.3 to 0.8
- forget_leak_rate: float32 [1024], P('tp'), may hold values from 2e-05 to 0.05
- extra_log_decay: float32 [1536, 1024], P('sp', 'tp'), may hold values from -1 to 0
- initial_recurrent_state: float32 [8, 128, 128], P('tp'), may hold values from -0.12 to 0.12
Outputs:
- mixer_out: bfloat16 [1536, 2048], P(('sp', 'tp'))
The draws below stay inside these ranges and needn't reach their ends.
All inputs are finite; a program needn't handle non-finite values.
Results may differ from the reference program's by a relative error of at most 0.014.
Values may be sent and summed in bfloat16 or wider, within the bound.
A program may use at most 128 MiB of HBM per device.

```python
import math
import jax
import jax.numpy as jnp
from jax import lax

D = 2048
DIFF_HEADS = 8
QK_DIM = 32
HEAD_DIM = 64
RECURRENT_HEADS = 8
RECURRENT_WIDTH = 128
REC_SPAN = 64
TOKEN_COUNT = 1536
N_TP = 4


def pair_raw(key):
    key_raw = jnp.clip(jax.random.normal(jax.random.fold_in(key, 101), (D, 2 * QK_DIM), jnp.float32), -4.0, 4.0)
    query_raw = jnp.clip(jax.random.normal(jax.random.fold_in(key, 102), (D, DIFF_HEADS * 2 * QK_DIM), jnp.float32), -4.0, 4.0)
    return (key_raw, query_raw)


def draw_shared_key_weight(key, part):
    key_raw, query_raw = pair_raw(key)
    return (key_raw * (2.0 / D) ** 0.5).astype(jnp.bfloat16)


def draw_paired_query_weight(key, part):
    key_raw, query_raw = pair_raw(key)
    weight_scale = (2.0 / D) ** 0.5
    return (query_raw * weight_scale).astype(jnp.bfloat16)


def draw_tokens(key, part):
    base_rows = jnp.clip(jax.random.normal(jax.random.fold_in(key, 201), (TOKEN_COUNT, D), jnp.float32), -6.0, 6.0)
    return base_rows.astype(jnp.bfloat16)


def draw_extra_log_decay(key, part):
    extra_decay_positions = jax.random.randint(jax.random.fold_in(key, 301), (8, RECURRENT_HEADS), 0, TOKEN_COUNT)
    row_position_index = jnp.arange(TOKEN_COUNT)
    extra_decay_flag = jnp.any(row_position_index[:, None, None] == extra_decay_positions[None], axis=1)
    extra_decay_depth = jax.random.uniform(jax.random.fold_in(key, 302), (TOKEN_COUNT, RECURRENT_HEADS), jnp.float32, jnp.log(0.5), jnp.log(0.8))
    extra_decay_field = jnp.where(extra_decay_flag, extra_decay_depth, 0.0)
    return jnp.repeat(extra_decay_field, RECURRENT_WIDTH, axis=1).astype(jnp.float32)


def block_scale(stream_key, extent, cuts, smallest, largest):
    factor_of, own = 1.0, jax.random.fold_in(stream_key, 6)
    for position, parts in cuts:
        heights = jnp.exp(jax.random.uniform(jax.random.fold_in(own, position), (parts,), jnp.float32, smallest / len(cuts), largest / len(cuts)))
        factor_of = factor_of * jnp.repeat(heights, extent[position] // parts).reshape([-1 if axis == position else 1 for axis in range(len(extent))])
    return factor_of


def centred(key, shape, deviation, reach, split=(), held_as=jnp.bfloat16):
    values = jax.random.normal(key, shape, jnp.float32) * deviation
    if len(split) > 0:
        values = block_scale(key, shape, split, -0.22, 0.18) * values
    return jnp.clip(values, min=-reach, max=reach).astype(held_as)


def setup_inputs(seed: int = 0) -> dict:
    seeds = jax.random.split(jax.random.key(seed), 17)
    return {
        "tokens": draw_tokens(jax.random.fold_in(seeds[16], 71), 0),
        "input_norm_gain": jnp.clip(1.0 + 0.18 * jax.random.normal(seeds[1], (D,), jnp.float32), 0.1, 1.9),
        "paired_query_weight": draw_paired_query_weight(jax.random.fold_in(seeds[16], 71), 0),
        "shared_key_weight": draw_shared_key_weight(jax.random.fold_in(seeds[16], 71), 0),
        "shared_value_weight": centred(seeds[4], (D, HEAD_DIM), D ** -0.5, 0.125),
        "recurrent_query_weight": centred(seeds[5], (D, RECURRENT_HEADS * RECURRENT_WIDTH), D ** -0.5, 0.125, ((0, 8), (1, 4))),
        "forget_gate_weight": centred(seeds[6], (D, RECURRENT_HEADS * RECURRENT_WIDTH), D ** -0.5, 0.125, ((0, 8), (1, 4))),
        "recurrent_value_weight": centred(seeds[7], (D, RECURRENT_HEADS * RECURRENT_WIDTH), D ** -0.5, 0.125, ((0, 8), (1, 4))),
        "attention_output_weight": centred(seeds[8], (D, DIFF_HEADS * HEAD_DIM), (DIFF_HEADS * HEAD_DIM + RECURRENT_HEADS * RECURRENT_WIDTH) ** -0.5, 0.15625, ((0, 8), (1, 4))),
        "recurrent_output_weight": centred(seeds[9], (D, RECURRENT_HEADS * RECURRENT_WIDTH), (DIFF_HEADS * HEAD_DIM + RECURRENT_HEADS * RECURRENT_WIDTH) ** -0.5, 0.15625, ((0, 8), (1, 4))),
        "attention_head_gain": jnp.clip(1.0 + 0.18 * jax.random.normal(seeds[10], (HEAD_DIM,), jnp.float32), 0.1, 1.9),
        "recurrent_head_gain": jnp.clip(1.0 + 0.18 * jax.random.normal(seeds[11], (RECURRENT_WIDTH,), jnp.float32), 0.1, 1.9),
        "second_map_weight": jnp.clip(0.3 + 0.5 * jax.random.uniform(seeds[12], (DIFF_HEADS,), jnp.float32) ** block_scale(seeds[12], (DIFF_HEADS,), ((0, 4),), -0.2, 0.2), 0.3, 0.8),
        "forget_leak_rate": jnp.clip(jnp.exp(math.log(0.05) - 7.824046 * jax.random.uniform(seeds[13], (RECURRENT_HEADS * RECURRENT_WIDTH,), jnp.float32) ** block_scale(seeds[13], (RECURRENT_HEADS * RECURRENT_WIDTH,), ((0, 4),), -0.2, 0.2)), 1.9999999494757503e-05, 0.05),
        "extra_log_decay": draw_extra_log_decay(jax.random.fold_in(seeds[16], 71), 0),
        "initial_recurrent_state": centred(seeds[15], (RECURRENT_HEADS, RECURRENT_WIDTH, RECURRENT_WIDTH), 0.02, 0.12, ((0, 4),), jnp.float32),
    }


epsilon = 1e-06

def rms_scale(matrix, gain):
    return matrix * lax.rsqrt(lax.optimization_barrier(jnp.mean(matrix * matrix, axis=-1, keepdims=True)) + epsilon) * gain

def project(normed, weight):
    return jnp.dot(normed, weight, preferred_element_type=jnp.float32).astype(jnp.bfloat16)

def widen(stored):
    return lax.optimization_barrier(stored).astype(jnp.float32)

def attend(queries, keys, values, second_map_weight, attention_head_gain):
    token_count = queries.shape[0]
    block_rows = math.gcd(token_count, 512)
    head_count = queries.shape[1] // (2 * QK_DIM)
    key_pair = keys.reshape(token_count, 2, QK_DIM)
    score_scale = 1.0 / math.sqrt(QK_DIM)

    def one_block(begin_row):
        query_rows = lax.dynamic_slice_in_dim(queries, begin_row, block_rows, 0).reshape(block_rows, head_count, 2, QK_DIM)
        head_outs = []
        for head_index in range(head_count):
            parts_list = []
            for component in range(2):
                scores = jnp.dot(query_rows[:, head_index, component], key_pair[:, component].T, preferred_element_type=jnp.float32) * score_scale
                peak_score = lax.optimization_barrier(jnp.max(scores, axis=1, keepdims=True))
                expo_terms = jnp.exp(scores - peak_score)
                totals = lax.optimization_barrier(jnp.sum(expo_terms, axis=1, keepdims=True))
                weighted = jnp.dot(expo_terms.astype(jnp.bfloat16), values, preferred_element_type=jnp.float32)
                parts_list.append(weighted / totals)
            blended = parts_list[0] - second_map_weight[head_index] * parts_list[1]
            head_outs.append(rms_scale(blended, attention_head_gain))
        return jnp.concatenate(head_outs, axis=1).astype(jnp.bfloat16)
    starts = jnp.arange(token_count // block_rows, dtype=jnp.int32) * block_rows
    pieces = lax.map(one_block, starts)
    return pieces.reshape(token_count, head_count * HEAD_DIM)

def recur_blocks(rec_query, inflow_state, rec_values, log_decay_values, initial):
    head_count, token_count, channel_width = rec_query.shape
    span_count = token_count // REC_SPAN

    def to_spans(matrix):
        return jnp.moveaxis(matrix.reshape(head_count, span_count, REC_SPAN, matrix.shape[-1]), 1, 0)
    lower_mask = jnp.tril(jnp.ones((REC_SPAN, REC_SPAN), jnp.float32))
    highest_precision = lax.Precision.HIGHEST

    def step(carried_state, inputs):
        query_span, inflow_span, value_segment, decay_span = inputs
        running = jnp.cumsum(decay_span, axis=1)
        segment_final = running[:, -1:, :]
        decayed_query = query_span * jnp.exp(running)
        inflow_dec = inflow_span * jnp.exp(-running)
        within_segment = jnp.einsum('hsk,htk->hst', decayed_query, inflow_dec, precision=highest_precision) * lower_mask
        segment_output = jnp.einsum('rcn,rni->rci', within_segment, value_segment, precision=highest_precision) + jnp.einsum('cwi,cip->cwp', decayed_query, carried_state, precision=highest_precision)
        inflow_final = inflow_span * jnp.exp(segment_final - running)
        carried_state = jnp.exp(segment_final)[:, 0, :, None] * carried_state + jnp.einsum('rgc,rgt->rct', inflow_final, value_segment, precision=highest_precision)
        return (carried_state, segment_output)
    final_state, span_outs = lax.scan(step, initial, (to_spans(rec_query), to_spans(inflow_state), to_spans(rec_values), to_spans(log_decay_values)))
    return jnp.moveaxis(span_outs, 0, 1).reshape(head_count, token_count, rec_values.shape[-1])

def reference(tokens, input_norm_gain, paired_query_weight, shared_key_weight, shared_value_weight, recurrent_query_weight, forget_gate_weight, recurrent_value_weight, attention_output_weight, recurrent_output_weight, attention_head_gain, recurrent_head_gain, second_map_weight, forget_leak_rate, extra_log_decay, initial_recurrent_state):
    token_count = tokens.shape[0]
    normed = rms_scale(tokens.astype(jnp.float32), input_norm_gain).astype(jnp.bfloat16)
    queries = project(normed, paired_query_weight)
    keys = project(normed, shared_key_weight)
    values = project(normed, shared_value_weight)
    attn_hidden = attend(queries, keys, values, second_map_weight, attention_head_gain)
    rec_query = jax.nn.silu(widen(project(normed, recurrent_query_weight)))
    gate_raw = widen(project(normed, forget_gate_weight))
    rec_values = widen(project(normed, recurrent_value_weight))
    inflow_state = forget_leak_rate * (1.0 - jax.nn.sigmoid(gate_raw))
    log_decay_values = jnp.log(1.0 - inflow_state) + extra_log_decay

    def heads_first(matrix):
        return matrix.reshape(token_count, RECURRENT_HEADS, RECURRENT_WIDTH).transpose(1, 0, 2)
    recurrent_output = recur_blocks(heads_first(rec_query), heads_first(inflow_state), heads_first(rec_values), heads_first(log_decay_values), initial_recurrent_state)
    rec_hidden = rms_scale(recurrent_output, recurrent_head_gain).transpose(1, 0, 2).reshape(token_count, RECURRENT_HEADS * RECURRENT_WIDTH)
    rec_hidden = rec_hidden.astype(jnp.bfloat16)
    attn_group = DIFF_HEADS * HEAD_DIM // N_TP
    rec_group = RECURRENT_HEADS * RECURRENT_WIDTH // N_TP
    summed = jnp.zeros((token_count, D), jnp.float32)
    for group_index in range(N_TP):
        attn_cols = slice(group_index * attn_group, (group_index + 1) * attn_group)
        rec_cols = slice(group_index * rec_group, (group_index + 1) * rec_group)
        group_part = jnp.dot(attn_hidden[:, attn_cols], attention_output_weight[:, attn_cols].T, preferred_element_type=jnp.float32) + jnp.dot(rec_hidden[:, rec_cols], recurrent_output_weight[:, rec_cols].T, preferred_element_type=jnp.float32)
        summed = summed + lax.optimization_barrier(group_part.astype(jnp.bfloat16)).astype(jnp.float32)
    return summed.astype(jnp.bfloat16)
```

```python
import functools
import math

import jax
import jax.numpy as jnp
from jax import lax
from jax.experimental import pallas as pl
from jax.experimental.pallas import tpu as pltpu
from jax.sharding import PartitionSpec as P

QK_DIM = 32
HEAD_DIM = 64
RECURRENT_WIDTH = 128
REC_SPAN = 64
KEY_BLOCK = 1536
OUT_WIDTH = 256
LAGS = (1, 3, 5)
EPS = 1e-06
MESH = pl.DeviceIdType.MESH
F32, BF16 = jnp.float32, jnp.bfloat16

NN = (((1,), (0,)), ((), ()))
NT = (((1,), (1,)), ((), ()))
TN = (((0,), (0,)), ((), ()))


def dot(a, b, dims=NN, precision=None):
    return lax.dot_general(a, b, dims, preferred_element_type=F32, precision=precision)


def rms(x, gain):
    return x * lax.rsqrt(jnp.mean(x * x, axis=-1, keepdims=True) + EPS) * gain


def loop(lo, hi, body):
    def step(j, carry):
        body(j)
        return carry

    lax.fori_loop(lo, hi, step, 0)


def kernel(
    n, nt,
    tok, gain, wq, wg, wv, wr, woa, wor, wk, wval, again, rgain, mapw, leak, extra, init,
    out,
    gb, pk, nf, kvb, xb, xs, st, sd, un, ud, pb, db, sb, yr, zb, zr,
    col_send, col_recv, row_send, row_recv, tg_send, tg_recv, kg_send, kg_recv,
    k1_send, k1_recv, x_send, x_recv, un_send, un_recv, ud_send, ud_recv,
    d_send, d_recv, y_send, y_recv, z_send, z_recv,
):
    s, t = lax.axis_index("sp"), lax.axis_index("tp")
    count_p, count_z, count_h = n // 2, n // 4, nt // 2
    small = count_p <= 4
    x, p = s % 2, s // 2
    zl, zh = p % 2, p // 2
    hi, lo = t // 2, t % 2
    zmate, xmate, cmate = s + 2 - 4 * zl, s + 1 - 2 * x, t + 1 - 2 * lo

    def remote(src, dst, send_sem, recv_sem, device):
        return pltpu.make_async_remote_copy(
            src_ref=src, dst_ref=dst, send_sem=send_sem, recv_sem=recv_sem,
            device_id=device, device_id_type=MESH,
        )

    barrier = pltpu.get_barrier_semaphore()

    def greet(peer):
        pl.semaphore_signal(barrier, inc=1, device_id=peer, device_id_type=MESH)

    loop(1, count_p, lambda j: greet((2 * ((p + j) % count_p) + x, t)))
    greet((xmate, t))
    greet((s, cmate))
    for k in range(1, count_h):
        greet((s, (t + 2 * k) % nt))

    rows, width = tok.shape
    part, half, w = wg.shape[0], wg.shape[0] // 2, RECURRENT_WIDTH
    at_v, at_r, at_q, at_a, at_o = part, 2 * part, 3 * part, 3 * part + half, 4 * part
    groups = ((0, at_v), (at_v, at_r), (at_r, at_a), (at_a, 5 * part))

    def split(ref, lo_row):
        mine = pl.ds(pl.multiple_of(zl * w, w), w)
        other = pl.ds(pl.multiple_of((1 - zl) * w, w), w)
        gb[s, lo_row : lo_row + part] = ref[:, mine]
        pk[lo_row : lo_row + part] = ref[:, other]

    def split_narrow(ref, lo_row):
        v = ref[...]
        a = v.shape[1] // 2
        first = jnp.concatenate([v[:half, :a], v[half:, :a]], axis=1)
        second = jnp.concatenate([v[:half, a:], v[half:, a:]], axis=1)
        gb[s, lo_row : lo_row + half] = jnp.where(zl == 0, first, second)
        pk[lo_row : lo_row + half] = jnp.where(zl == 0, second, first)

    split(wg, 0)
    split(wv, at_v)
    split(wr, at_r)
    split_narrow(wq, at_q)
    split_narrow(woa, at_a)
    split(wor, at_o)
    xb[zl] = extra[:, pl.ds(pl.multiple_of(zl * w, w), w)]
    xs[...] = extra[:, pl.ds(pl.multiple_of((1 - zl) * w, w), w)]

    normed = rms(tok[...].astype(F32), gain[...]).astype(BF16)
    nf[zl, t] = normed
    kvb[zl, t, x, zh] = jnp.concatenate(
        [dot(normed, wk[...], NT).astype(BF16), dot(normed, wval[...], NT).astype(BF16)], axis=1
    )
    pl.semaphore_wait(barrier, count_p + count_h)

    class Gather:
        def __init__(self, ref, send, recv):
            self.ref, self.send, self.recv = ref, send, recv

        def slot(self, zz, owner):
            return self.ref.at[zl if zz == 0 else 1 - zl, owner % nt]

        def copy(self, kind, zz, k, owner, device):
            block = self.slot(zz, owner)
            return remote(block, block, self.send.at[kind, zz, k], self.recv.at[kind, zz, k], device)

        def core_out(self, zz, k):
            return self.copy(0, zz, k, t + nt - 2 * k, (s, cmate))

        def core_in(self, zz, k):
            return self.copy(0, zz, k, cmate + nt - 2 * k, (s, cmate))

        def y_out(self, zz, k):
            return self.copy(1, zz, k, t, (s, (t + 2 * k) % nt))

        def y_in(self, zz, k):
            return self.copy(1, zz, k, t + nt - 2 * k, (s, (t + nt - 2 * k) % nt))

        def z_out(self):
            return self.copy(2, 0, 0, t, (zmate, t))

        def z_in(self):
            block = self.slot(1, t)
            return remote(block, block, self.send.at[2, 0, 0], self.recv.at[2, 0, 0], (zmate, t))

        def start(self):
            self.z_out().start()
            for k in range(1, count_h):
                self.y_out(0, k).start()
            self.core_out(0, 0).start()

        def relay_z(self):
            self.z_in().wait_recv()
            for k in range(1, count_h):
                self.y_out(1, k).start()
            self.core_out(1, 0).start()

        def relay_y(self, zz):
            for k in range(1, count_h):
                self.y_in(zz, k).wait_recv()
                self.core_out(zz, k).start()

        def arrive(self):
            for zz in (0, 1):
                for k in range(count_h):
                    self.core_in(zz, k).wait_recv()

        def finish(self):
            self.z_out().wait_send()
            for zz in (0, 1):
                for k in range(count_h):
                    self.core_out(zz, k).wait_send()
                    if k > 0:
                        self.y_out(zz, k).wait_send()

    tokens, keyvals = Gather(nf, tg_send, tg_recv), Gather(kvb, kg_send, kg_recv)

    def cut(ref, g):
        return ref.at[groups[g][0] : groups[g][1]]

    def col_out(p2, g, same):
        return remote(
            cut(gb.at[s], g) if same else cut(pk, g), cut(gb.at[s], g),
            col_send.at[p2, g], col_recv.at[p, g], (2 * p2 + x, t),
        )

    def col_in(p2, g):
        slot = cut(gb.at[2 * p2 + x], g)
        return remote(slot, slot, col_send.at[p2, g], col_recv.at[p2, g], (2 * p2 + x, t))

    def row_out(p2, g):
        slot = cut(gb.at[2 * p2 + x], g)
        return remote(slot, slot, row_send.at[p2, g], row_recv.at[p2, g], (xmate, t))

    def row_in(p2, g):
        slot = cut(gb.at[2 * p2 + 1 - x], g)
        return remote(slot, slot, row_send.at[p2, g], row_recv.at[p2, g], (xmate, t))

    def near(d, body):
        for sign in (1, -1):
            p2 = p + sign * d

            @pl.when((p2 >= 0) & (p2 < count_p))
            def _():
                body(p2)

    def distances(body):
        if small:
            for d in range(1, count_p):
                body(d, d % 2 == 0)
        else:
            loop(0, count_p // 2, lambda i: body(2 * i + 1, False))
            loop(1, count_p // 2, lambda i: body(2 * i, True))

    def issue(g, d):
        if d == 1:
            row_out(p, g).start()
        if small:
            near(d, lambda p2: col_out(p2, g, d % 2 == 0).start())
        elif d == 1:
            distances(lambda e, same: near(e, lambda p2: col_out(p2, g, same).start()))

    def forward_one(g, p2):
        col_in(p2, g).wait_recv()
        row_out(p2, g).start()

    def forward(g, d):
        if small:
            near(d, lambda p2: forward_one(g, p2))
        elif d == 1:
            loop(1, count_p, lambda e: near(e, lambda p2: forward_one(g, p2)))

    def collect(g):
        loop(0, count_p, lambda p2: row_in(p2, g).wait_recv())

    def finish(g):
        distances(lambda d, same: near(d, lambda p2: col_out(p2, g, same).wait_send()))
        loop(0, count_p, lambda p2: row_out(p2, g).wait_send())

    def k1_copy(j, owner):
        block = kvb.at[zl, t, x, owner % count_z]
        peer = (zh + j) % count_z
        return remote(block, block, k1_send.at[j], k1_recv.at[j], (4 * peer + 2 * zl + x, t))

    def swap(i, src, dst, device):
        return remote(src, dst, x_send.at[i], x_recv.at[i], device)

    def kv_swap(side):
        return swap(0, kvb.at[zl, t, side], kvb.at[zl, t, side], (xmate, t))

    def extra_swap(side):
        return swap(1, xs, xb.at[side], (zmate, t))

    def st_swap(side):
        return swap(2, st.at[side], st.at[side], (xmate, t))

    def sd_swap(side):
        return swap(3, sd.at[side], sd.at[side], (xmate, t))

    loop(1, count_z, lambda j: k1_copy(j, zh).start())
    issue(0, 1)
    tokens.start()
    issue(0, 2)
    issue(0, 3)
    for d in (1, 2, 3):
        issue(1, d)
    extra_swap(zl).start()
    forward(0, 1)
    tokens.relay_y(0)
    loop(1, count_z, lambda j: k1_copy(j, zh + count_z - j).wait_recv())
    kv_swap(x).start()
    tokens.relay_z()
    forward(0, 2)
    forward(1, 1)
    kv_swap(1 - x).wait_recv()
    keyvals.start()
    forward(0, 3)
    for d in (1, 2, 3):
        issue(2, d)
    tokens.relay_y(1)
    forward(1, 2)
    forward(1, 3)
    tokens.arrive()
    extra_swap(1 - zl).wait_recv()
    collect(0)

    block = nt * rows
    full = nf[...].reshape(2 * block, width)

    def weight(lo_row):
        return gb[:, lo_row : lo_row + part].reshape(n * part, w)

    def widen(v):
        a = v.shape[2] // 2
        both = jnp.concatenate([v[:, :, :a], v[:, :, a:]], axis=1)
        return both.reshape(both.shape[0] * both.shape[1], a)

    gate = dot(full, weight(0)).astype(BF16).astype(F32)
    forward(2, 1)

    leak_mine = jnp.where(zl == 0, leak[:, :w], leak[:, w:])
    inflow = leak_mine * (1.0 - jax.nn.sigmoid(gate))
    log_decay = jnp.log(1.0 - inflow) + xb[...].reshape(2 * block, w)
    spans = block // REC_SPAN
    rr = lax.broadcasted_iota(jnp.int32, (REC_SPAN, REC_SPAN), 0)
    cc = lax.broadcasted_iota(jnp.int32, (REC_SPAN, REC_SPAN), 1)
    lower = (rr >= cc).astype(F32)
    running, offsets, befores, weighted = [], [], [], []
    for j in (0, 1):
        offset = jnp.zeros((1, w), F32)
        for i in range(spans):
            r = slice(j * block + i * REC_SPAN, j * block + (i + 1) * REC_SPAN)
            run = dot(lower, log_decay[r], precision=lax.Precision.HIGHEST)
            final = run[REC_SPAN - 1 : REC_SPAN]
            running.append(run)
            offsets.append(offset)
            offset = offset + final
            weighted.append((inflow[r] * jnp.exp(final - run)).astype(BF16))
        sd[x, j] = jnp.broadcast_to(offset, sd.shape[2:])
    collect(1)
    vals = dot(full, weight(at_v)).astype(BF16)
    for j in (0, 1):
        carried = None
        for i in range(spans):
            r = slice(j * block + i * REC_SPAN, j * block + (i + 1) * REC_SPAN)
            final = running[j * spans + i][REC_SPAN - 1 : REC_SPAN]
            befores.append(carried)
            new = dot(vals[r], weighted[j * spans + i], TN)
            carried = new if carried is None else carried * jnp.exp(final) + new
        st[x, j] = carried.astype(BF16)
    st_swap(x).start()
    sd_swap(x).start()

    forward(2, 2)

    def advance(carried, sx, j):
        return carried * jnp.exp(sd[sx, j][0:1]) + st[sx, j].astype(F32)

    def un_pair(z2, owner):
        device = (4 * z2 + 2 * zl + x, t)
        return (
            remote(un.at[owner], un.at[owner], un_send.at[z2], un_recv.at[owner], device),
            remote(ud.at[owner], ud.at[owner], ud_send.at[z2], ud_recv.at[owner], device),
        )

    def un_start(z2):
        for copy in un_pair(z2, zh):
            copy.start()

    def un_wait(owner):
        for copy in un_pair(owner, owner):
            copy.wait_recv()

    def join_units():
        st_swap(1 - x).wait_recv()
        sd_swap(1 - x).wait_recv()
        unit = st[0, 0].astype(F32)
        for sx, j in ((1, 0), (0, 1), (1, 1)):
            unit = advance(unit, sx, j)
        un[zh] = unit.astype(BF16)
        ud[zh] = sd[0, 0] + sd[1, 0] + sd[0, 1] + sd[1, 1]
        loop(zh + 1, count_z, un_start)

    def un_done(z2):
        for copy in un_pair(z2, zh):
            copy.wait_send()

    keyvals.relay_z()
    keyvals.relay_y(0)
    for d in (1, 2, 3):
        issue(3, d)
    forward(2, 3)
    keyvals.relay_y(1)
    collect(2)
    keyvals.arrive()

    raw = dot(full, weight(at_r)).astype(BF16).astype(F32)
    queries = dot(full, widen(gb[:, at_q:at_a])).astype(BF16)

    zs = max(1, min(count_z, KEY_BLOCK // (4 * block)))
    blocks = count_z // zs
    scale = 1.0 / math.sqrt(QK_DIM)

    def attend(query, b):
        both = kvb[:, :, :, pl.ds(b * zs, zs)].reshape(4 * zs * block, kvb.shape[5])
        values = both[:, 2 * QK_DIM :]
        parts = []
        for comp in range(2):
            cols = slice(comp * QK_DIM, (comp + 1) * QK_DIM)
            scores = dot(query[:, cols], both[:, cols], NT) * scale
            peak = jnp.max(scores, axis=1, keepdims=True)
            expo = jnp.exp(scores - peak)
            parts += [peak, jnp.sum(expo, axis=1, keepdims=True), dot(expo.astype(BF16), values)]
        return tuple(parts)

    def merge(a, b):
        parts = []
        for comp in range(2):
            pa, ta, wa = a[3 * comp : 3 * comp + 3]
            pc, tc, wc = b[3 * comp : 3 * comp + 3]
            peak = jnp.maximum(pa, pc)
            ea, ec = jnp.exp(pa - peak), jnp.exp(pc - peak)
            parts += [peak, ta * ea + tc * ec, wa * ea + wc * ec]
        return tuple(parts)

    hidden = []
    for j in (0, 1):
        query = queries[j * block : (j + 1) * block]
        got = attend(query, 0)
        if blocks > 1:
            got = lax.fori_loop(1, blocks, lambda b, g: merge(g, attend(query, b)), got)
        blended = got[2] / got[1] - mapw[zl] * (got[5] / got[4])
        hidden.append(rms(blended, again[...]))
        forward(3, 1 + j)
        if j == 0:
            join_units()
    attn_hidden = jnp.concatenate(hidden, axis=0).astype(BF16)

    rec_query = raw * jax.nn.sigmoid(raw)
    local, lifted = [], []
    for j in (0, 1):
        outs, lifts = [], []
        for i in range(spans):
            r = slice(j * block + i * REC_SPAN, j * block + (i + 1) * REC_SPAN)
            run = running[j * spans + i]
            before = befores[j * spans + i]
            dq = (rec_query[r] * jnp.exp(run)).astype(BF16)
            within = dot(dq, (inflow[r] * jnp.exp(-run)).astype(BF16), NT) * lower
            o = dot(within.astype(BF16), vals[r])
            if before is not None:
                o = o + dot(dq, before.astype(BF16), NT)
            outs.append(o)
            lifts.append(rec_query[r] * jnp.exp(offsets[j * spans + i] + run))
        local.append(jnp.concatenate(outs, axis=0))
        lifted.append(jnp.concatenate(lifts, axis=0).astype(BF16))

    loop(0, zh, un_wait)

    def chain(k, carry):
        return carry * jnp.exp(ud[k][0:1]) + un[k].astype(F32)

    base = lax.fori_loop(0, zh, chain, init[zl].T)
    s01 = advance(base, 0, 0)
    s10 = advance(s01, 1, 0)
    s11 = advance(s10, 0, 1)
    incoming = (jnp.where(x == 0, base, s01), jnp.where(x == 0, s10, s11))
    rec = []
    for j in (0, 1):
        o = local[j] + dot(lifted[j], incoming[j].astype(BF16), NT)
        rec.append(rms(o, rgain[...]))
    rec_hidden = jnp.concatenate(rec, axis=0).astype(BF16)
    both_hidden = jnp.concatenate([rec_hidden, attn_hidden], axis=1)

    per = pb.shape[5] // part
    fw = per * part
    chunks = n // per

    def d_copy(ch):
        return remote(pb.at[ch, 1 - lo], db.at[ch], d_send.at[ch], d_recv.at[ch], (s, cmate))

    def y_copy(ch, k, flip):
        h2 = (hi + k) % count_h
        src = zb.at[ch, pl.ds(h2, 1)] if flip else sb.at[ch, pl.ds(2 * h2, 2)]
        dst = yr.at[ch, k, pl.ds(0, 1)] if flip else yr.at[ch, k]
        return remote(src, dst, y_send.at[ch, k], y_recv.at[ch, k], (s, 2 * h2 + lo))

    def z_copy(ch, flip):
        src = sb.at[ch, pl.ds(count_h * (1 - zl), count_h)] if flip else zb.at[ch, pl.ds(1 - zl, 1)]
        dst = zr.at[ch] if flip else zr.at[ch, pl.ds(0, 1)]
        return remote(src, dst, z_send.at[ch], z_recv.at[ch], (zmate, t))

    def stage_d(ch):
        shard = gb[pl.ds(ch * per, per)]
        weights = jnp.concatenate(
            [shard[:, at_o:].reshape(fw, w), widen(shard[:, at_a:at_o])], axis=1
        )
        got = dot(both_hidden, weights, NT).astype(BF16)
        for z2 in (0, 1):
            for t2 in range(nt):
                lo_row = (z2 * nt + t2) * rows
                pb[ch, t2 % 2, z2, t2 // 2] = got[lo_row : lo_row + rows]
        d_copy(ch).start()

    def stage_first(ch, flip):
        d_copy(ch).wait_recv()
        total = (pb[ch, lo].astype(F32) + db[ch].astype(F32)).astype(BF16)
        if flip:
            sb[ch] = total.reshape(sb.shape[1:])
            z_copy(ch, flip).start()
        else:
            for h2 in range(count_h):
                sb[ch, 2 * h2 : 2 * h2 + 2] = total[:, h2]
            for k in range(1, count_h):
                y_copy(ch, k, flip).start()

    def stage_second(ch, flip):
        if flip:
            z_copy(ch, flip).wait_recv()
            mine = sb[ch, pl.ds(count_h * zl, count_h)]
            zb[ch] = (mine.astype(F32) + zr[ch].astype(F32)).astype(BF16)
            for k in range(1, count_h):
                y_copy(ch, k, flip).start()
        else:
            total = sb[ch, pl.ds(2 * hi, 2)].astype(F32)
            for k in range(1, count_h):
                y_copy(ch, k, flip).wait_recv()
                total = total + yr[ch, k].astype(F32)
            zb[ch, 0:2] = total.astype(BF16)
            z_copy(ch, flip).start()

    def stage_out(ch, flip):
        if flip:
            total = zb[ch, hi].astype(F32)
            for k in range(1, count_h):
                y_copy(ch, k, flip).wait_recv()
                total = total + yr[ch, k, 0].astype(F32)
        else:
            z_copy(ch, flip).wait_recv()
            total = zb[ch, zl].astype(F32) + zr[ch, 0].astype(F32)
        out[:, pl.ds(pl.multiple_of(ch * fw, fw), fw)] = total.astype(out.dtype)

    if small and per == 1:
        order = []
        for k in range(count_z):
            z2 = (zh + k) % count_z
            pair = (2 * z2, 2 * z2 + 1)
            order += [(q, c) for c in (0, 1) for q in pair] if k == 0 else [(q, c) for q in pair for c in (0, 1)]
        forward(3, 3)
        ready = []
        for q, c in order:
            ready.append((2 * q + x if c == 0 else 2 * q + 1 - x, q if c == 1 else None))
    else:
        collect(3)
        ready = [(ch, None) for ch in range(chunks)]

    lag = len(ready)
    for i in range(lag + LAGS[2]):
        if i < lag:
            ch, q = ready[i]
            if q is not None:
                row_in(q, 3).wait_recv()
            stage_d(ch)
        for body, late in zip((stage_first, stage_second, stage_out), LAGS):
            if 0 <= i - late < lag:
                body(ready[i - late][0], (i - late) % 2 == 1)

    for g in (0, 1, 2, 3):
        finish(g)
    tokens.finish()
    keyvals.finish()
    loop(1, count_z, lambda j: k1_copy(j, zh).wait_send())
    kv_swap(x).wait_send()
    extra_swap(zl).wait_send()
    st_swap(x).wait_send()
    sd_swap(x).wait_send()
    loop(zh + 1, count_z, un_done)

    for i, (ch, _) in enumerate(ready):
        d_copy(ch).wait_send()
        for k in range(1, count_h):
            y_copy(ch, k, i % 2 == 1).wait_send()
        z_copy(ch, i % 2 == 1).wait_send()


def solution(mesh):
    n, nt = mesh.shape["sp"], mesh.shape["tp"]

    def body(
        tokens, input_norm_gain, paired_query_weight, shared_key_weight, shared_value_weight,
        recurrent_query_weight, forget_gate_weight, recurrent_value_weight,
        attention_output_weight, recurrent_output_weight, attention_head_gain,
        recurrent_head_gain, second_map_weight, forget_leak_rate, extra_log_decay,
        initial_recurrent_state,
    ):
        rows, width = tokens.shape
        weights = (
            paired_query_weight, forget_gate_weight, recurrent_value_weight,
            recurrent_query_weight, attention_output_weight, recurrent_output_weight,
        )
        part = forget_gate_weight.shape[0]
        span = extra_log_decay.shape[0]
        count_p, count_z, count_h = n // 2, n // 4, nt // 2
        fw = part * max(1, OUT_WIDTH // part)
        chunks = width // fw
        kv_width = 2 * QK_DIM + HEAD_DIM
        vm = pl.BlockSpec(memory_space=pltpu.VMEM)
        sm = pl.BlockSpec(memory_space=pltpu.SMEM)
        dma = pltpu.SemaphoreType.DMA
        w = RECURRENT_WIDTH
        return pl.pallas_call(
            functools.partial(kernel, n, nt),
            out_shape=jax.ShapeDtypeStruct((rows, width), BF16),
            in_specs=[vm] * 12 + [sm] + [vm] * 3,
            out_specs=vm,
            scratch_shapes=[
                pltpu.VMEM((n, 5 * part, w), BF16),
                pltpu.VMEM((5 * part, w), BF16),
                pltpu.VMEM((2, nt, rows, width), BF16),
                pltpu.VMEM((2, nt, 2, count_z, rows, kv_width), BF16),
                pltpu.VMEM((2, span, w), F32),
                pltpu.VMEM((span, w), F32),
                pltpu.VMEM((2, 2, w, w), BF16),
                pltpu.VMEM((2, 2, 8, w), F32),
                pltpu.VMEM((count_z, w, w), BF16),
                pltpu.VMEM((count_z, 8, w), F32),
                pltpu.VMEM((chunks, 2, 2, count_h, rows, fw), BF16),
                pltpu.VMEM((chunks, 2, count_h, rows, fw), BF16),
                pltpu.VMEM((chunks, 2 * count_h, rows, fw), BF16),
                pltpu.VMEM((chunks, count_h, 2, rows, fw), BF16),
                pltpu.VMEM((chunks, max(2, count_h), rows, fw), BF16),
                pltpu.VMEM((chunks, max(2, count_h), rows, fw), BF16),
                dma((count_p, 4)), dma((count_p, 4)),
                dma((count_p, 4)), dma((count_p, 4)),
                dma((3, 2, count_h)), dma((3, 2, count_h)),
                dma((3, 2, count_h)), dma((3, 2, count_h)),
                dma((count_z,)), dma((count_z,)),
                dma((4,)), dma((4,)),
                dma((count_z,)), dma((count_z,)),
                dma((count_z,)), dma((count_z,)),
                dma((chunks,)), dma((chunks,)),
                dma((chunks, count_h)), dma((chunks, count_h)),
                dma((chunks,)), dma((chunks,)),
            ],
            compiler_params=pltpu.CompilerParams(
                has_side_effects=True, collective_id=0, vmem_limit_bytes=60 * 1024 * 1024
            ),
        )(
            tokens, input_norm_gain[None], *weights, shared_key_weight.T, shared_value_weight.T,
            attention_head_gain[None], recurrent_head_gain[None], second_map_weight,
            forget_leak_rate[None], extra_log_decay, initial_recurrent_state,
        )

    placed = (
        P(("sp", "tp"), None), P(), P("sp", "tp"), P(), P(), P("sp", "tp"), P("sp", "tp"),
        P("sp", "tp"), P("sp", "tp"), P("sp", "tp"), P(), P(), P("tp"), P("tp"),
        P("sp", "tp"), P("tp", None, None),
    )
    return jax.shard_map(
        body, mesh=mesh, in_specs=placed, out_specs=P(("sp", "tp"), None), check_vma=False
    )
```

```python
import functools
import math

import jax
import jax.numpy as jnp
from jax import lax
from jax.experimental import pallas as pl
from jax.experimental.pallas import tpu as pltpu
from jax.sharding import PartitionSpec as P

QK_DIM = 32
HEAD_DIM = 64
RECURRENT_WIDTH = 128
REC_SPAN = 64
KEY_BLOCK = 1536
OUT_WIDTH = 256
LAGS = (2, 5, 8)
EPS = 1e-06
MESH = pl.DeviceIdType.MESH
F32, BF16 = jnp.float32, jnp.bfloat16

NN = (((1,), (0,)), ((), ()))
NT = (((1,), (1,)), ((), ()))
TN = (((0,), (0,)), ((), ()))


def dot(a, b, dims=NN, precision=None):
    return lax.dot_general(a, b, dims, preferred_element_type=F32, precision=precision)


def rms(x, gain):
    return x * lax.rsqrt(jnp.mean(x * x, axis=-1, keepdims=True) + EPS) * gain


def loop(lo, hi, body):
    def step(j, carry):
        body(j)
        return carry

    lax.fori_loop(lo, hi, step, 0)


def kernel(
    n, nt,
    tok_in, gain, wq_in, wg_in, wv_in, wr_in, woa_in, wor_in, wk_in, wval_in, again, rgain, mapw, leak,
    extra_in, init_in,
    out_ref,
    tok, wq, wg, wv, wr, woa, wor, wk, wval, extra, init, out, in_sem, out_sem,
    gb, pk, nf, kvb, xb, xs, st, sd, un, ud, pb, db, sb, yr, zb, zr,
    col_send, col_recv, row_send, row_recv, tg_send, tg_recv, kg_send, kg_recv,
    k1_send, k1_recv, x_send, x_recv, un_send, un_recv, ud_send, ud_recv,
    d_send, d_recv, y_send, y_recv, z_send, z_recv,
):
    s, t = lax.axis_index("sp"), lax.axis_index("tp")
    count_p, count_z, count_h = n // 2, n // 4, nt // 2
    small = count_p <= 4
    x, p = s % 2, s // 2
    zl, zh = p % 2, p // 2
    hi, lo = t // 2, t % 2
    zmate, xmate, cmate = s + 2 - 4 * zl, s + 1 - 2 * x, t + 1 - 2 * lo

    def remote(src, dst, send_sem, recv_sem, device):
        return pltpu.make_async_remote_copy(
            src_ref=src, dst_ref=dst, send_sem=send_sem, recv_sem=recv_sem,
            device_id=device, device_id_type=MESH,
        )

    order_in = (
        (tok_in, tok), (wg_in, wg), (wv_in, wv), (wq_in, wq), (wr_in, wr), (woa_in, woa),
        (wor_in, wor), (extra_in, extra), (wk_in, wk), (wval_in, wval), (init_in, init),
    )
    loads = [pltpu.make_async_copy(a, b, in_sem.at[i]) for i, (a, b) in enumerate(order_in)]
    for load in loads:
        load.start()
    barrier = pltpu.get_barrier_semaphore()

    def greet(peer):
        pl.semaphore_signal(barrier, inc=1, device_id=peer, device_id_type=MESH)

    loop(1, count_p, lambda j: greet((2 * ((p + j) % count_p) + x, t)))
    greet((xmate, t))
    greet((s, cmate))
    for k in range(1, count_h):
        greet((s, (t + 2 * k) % nt))

    for load in loads:
        load.wait()

    rows, width = tok.shape
    part, half, w = wg.shape[0], wg.shape[0] // 2, RECURRENT_WIDTH
    at_v, at_q, at_r, at_a, at_o = part, 2 * part, 2 * part + half, 3 * part + half, 4 * part
    groups = ((0, at_v), (at_v, at_r), (at_r, at_a), (at_a, 5 * part))

    def split(ref, lo_row):
        mine = pl.ds(pl.multiple_of(zl * w, w), w)
        other = pl.ds(pl.multiple_of((1 - zl) * w, w), w)
        gb[s, lo_row : lo_row + part] = ref[:, mine]
        pk[lo_row : lo_row + part] = ref[:, other]

    def split_narrow(ref, lo_row):
        v = ref[...]
        a = v.shape[1] // 2
        first = jnp.concatenate([v[:half, :a], v[half:, :a]], axis=1)
        second = jnp.concatenate([v[:half, a:], v[half:, a:]], axis=1)
        gb[s, lo_row : lo_row + half] = jnp.where(zl == 0, first, second)
        pk[lo_row : lo_row + half] = jnp.where(zl == 0, second, first)

    split(wg, 0)
    split(wv, at_v)
    split(wr, at_r)
    split_narrow(wq, at_q)
    split_narrow(woa, at_a)
    split(wor, at_o)
    xs[...] = extra[:, pl.ds(pl.multiple_of((1 - zl) * w, w), w)].astype(BF16)

    normed = rms(tok[...].astype(F32), gain[...]).astype(BF16)
    nf[zl, t] = normed
    kvb[zl, t, x, zh] = jnp.concatenate(
        [dot(normed, wk[...], NT).astype(BF16), dot(normed, wval[...], NT).astype(BF16)], axis=1
    )
    pl.semaphore_wait(barrier, count_p + count_h)

    class Gather:
        def __init__(self, ref, send, recv):
            self.ref, self.send, self.recv = ref, send, recv

        def slot(self, zz, owner):
            return self.ref.at[zl if zz == 0 else 1 - zl, owner % nt]

        def copy(self, kind, zz, k, owner, device):
            block = self.slot(zz, owner)
            return remote(block, block, self.send.at[kind, zz, k], self.recv.at[kind, zz, k], device)

        def core_out(self, zz, k):
            return self.copy(0, zz, k, t + nt - 2 * k, (s, cmate))

        def core_in(self, zz, k):
            return self.copy(0, zz, k, cmate + nt - 2 * k, (s, cmate))

        def y_out(self, zz, k):
            return self.copy(1, zz, k, t, (s, (t + 2 * k) % nt))

        def y_in(self, zz, k):
            return self.copy(1, zz, k, t + nt - 2 * k, (s, (t + nt - 2 * k) % nt))

        def z_out(self):
            return self.copy(2, 0, 0, t, (zmate, t))

        def z_in(self):
            block = self.slot(1, t)
            return remote(block, block, self.send.at[2, 0, 0], self.recv.at[2, 0, 0], (zmate, t))

        def start(self):
            self.z_out().start()
            for k in range(1, count_h):
                self.y_out(0, k).start()
            self.core_out(0, 0).start()

        def relay_z(self):
            self.z_in().wait_recv()
            for k in range(1, count_h):
                self.y_out(1, k).start()
            self.core_out(1, 0).start()

        def relay_y(self, zz):
            for k in range(1, count_h):
                self.y_in(zz, k).wait_recv()
                self.core_out(zz, k).start()

        def arrive(self):
            for zz in (0, 1):
                for k in range(count_h):
                    self.core_in(zz, k).wait_recv()

        def finish(self):
            self.z_out().wait_send()
            for zz in (0, 1):
                for k in range(count_h):
                    self.core_out(zz, k).wait_send()
                    if k > 0:
                        self.y_out(zz, k).wait_send()

    tokens, keyvals = Gather(nf, tg_send, tg_recv), Gather(kvb, kg_send, kg_recv)

    def cut(ref, g):
        return ref.at[groups[g][0] : groups[g][1]]

    def col_out(p2, g, same):
        return remote(
            cut(gb.at[s], g) if same else cut(pk, g), cut(gb.at[s], g),
            col_send.at[p2, g], col_recv.at[p, g], (2 * p2 + x, t),
        )

    def col_in(p2, g):
        slot = cut(gb.at[2 * p2 + x], g)
        return remote(slot, slot, col_send.at[p2, g], col_recv.at[p2, g], (2 * p2 + x, t))

    def row_out(p2, g):
        slot = cut(gb.at[2 * p2 + x], g)
        return remote(slot, slot, row_send.at[p2, g], row_recv.at[p2, g], (xmate, t))

    def row_in(p2, g):
        slot = cut(gb.at[2 * p2 + 1 - x], g)
        return remote(slot, slot, row_send.at[p2, g], row_recv.at[p2, g], (xmate, t))

    def near(d, body):
        for sign in (1, -1):
            p2 = p + sign * d

            @pl.when((p2 >= 0) & (p2 < count_p))
            def _():
                body(p2)

    def distances(body):
        if small:
            for d in range(1, count_p):
                body(d, d % 2 == 0)
        else:
            loop(0, count_p // 2, lambda i: body(2 * i + 1, False))
            loop(1, count_p // 2, lambda i: body(2 * i, True))

    def columns(g):
        distances(lambda d, same: near(d, lambda p2: col_out(p2, g, same).start()))

    sources = (count_z - zh, p + 1 - 2 * zl, (count_p - 1) * (1 - zh))

    def forward_one(g, p2):
        col_in(p2, g).wait_recv()
        row_out(p2, g).start()

    def forward(g, i):
        if small:
            forward_one(g, sources[i])
        elif i == 0:
            loop(1, count_p, lambda e: near(e, lambda p2: forward_one(g, p2)))

    at_edge = (p == 0) | (p == count_p - 1)

    def at_end(body):
        if small:
            pl.when(at_edge)(body)

    def at_middle(body):
        if small:
            pl.when(jnp.logical_not(at_edge))(body)
        else:
            body()

    def collect(g):
        loop(0, count_p, lambda p2: row_in(p2, g).wait_recv())

    def finish(g):
        distances(lambda d, same: near(d, lambda p2: col_out(p2, g, same).wait_send()))
        loop(0, count_p, lambda p2: row_out(p2, g).wait_send())

    def k1_copy(j, owner):
        block = kvb.at[zl, t, x, owner % count_z]
        peer = (zh + j) % count_z
        return remote(block, block, k1_send.at[j], k1_recv.at[j], (4 * peer + 2 * zl + x, t))

    def swap(i, src, dst, device):
        return remote(src, dst, x_send.at[i], x_recv.at[i], device)

    def kv_swap(side):
        return swap(0, kvb.at[zl, t, side], kvb.at[zl, t, side], (xmate, t))

    def extra_swap():
        return swap(1, xs, xb, (zmate, t))

    def st_swap(side):
        return swap(2, st.at[side], st.at[side], (xmate, t))

    def sd_swap(side):
        return swap(3, sd.at[side], sd.at[side], (xmate, t))

    loop(1, count_z, lambda j: k1_copy(j, zh).start())
    tokens.start()
    row_out(p, 0).start()
    row_out(p, 1).start()
    columns(0)
    columns(1)
    extra_swap().start()
    loop(1, count_z, lambda j: k1_copy(j, zh + count_z - j).wait_recv())
    kv_swap(x).start()
    row_out(p, 2).start()
    row_out(p, 3).start()
    forward(0, 0)
    kv_swap(1 - x).wait_recv()
    keyvals.start()
    columns(2)
    tokens.relay_y(0)
    tokens.relay_z()
    at_middle(lambda: forward(1, 0))
    forward(0, 1)
    forward(0, 2)
    forward(1, 1)
    at_end(lambda: forward(1, 0))
    tokens.relay_y(1)
    forward(1, 2)
    columns(3)
    keyvals.relay_z()
    keyvals.relay_y(0)
    at_middle(lambda: forward(2, 0))
    at_middle(lambda: forward(2, 1))
    tokens.arrive()
    extra_swap().wait_recv()
    collect(0)

    block = nt * rows
    full = nf[...].reshape(2 * block, width)

    def weight(lo_row):
        return gb[:, lo_row : lo_row + part].reshape(n * part, w)

    def widen(v):
        a = v.shape[2] // 2
        both = jnp.concatenate([v[:, :, :a], v[:, :, a:]], axis=1)
        return both.reshape(both.shape[0] * both.shape[1], a)

    gate = dot(full, weight(0)).astype(BF16).astype(F32)
    leak_mine = jnp.where(zl == 0, leak[:, :w], leak[:, w:])
    inflow = leak_mine * (1.0 - jax.nn.sigmoid(gate))
    here = extra[:, pl.ds(pl.multiple_of(zl * w, w), w)]
    there = xb[...].astype(F32)
    added = jnp.concatenate([jnp.where(zl == 0, here, there), jnp.where(zl == 0, there, here)], axis=0)
    log_decay = jnp.log(1.0 - inflow) + added
    spans = block // REC_SPAN
    rr = lax.broadcasted_iota(jnp.int32, (REC_SPAN, REC_SPAN), 0)
    cc = lax.broadcasted_iota(jnp.int32, (REC_SPAN, REC_SPAN), 1)
    lower = (rr >= cc).astype(F32)
    running, offsets, befores, weighted = [], [], [], []
    for j in (0, 1):
        offset = jnp.zeros((1, w), F32)
        for i in range(spans):
            r = slice(j * block + i * REC_SPAN, j * block + (i + 1) * REC_SPAN)
            run = dot(lower, log_decay[r], precision=lax.Precision.HIGHEST)
            final = run[REC_SPAN - 1 : REC_SPAN]
            running.append(run)
            offsets.append(offset)
            offset = offset + final
            weighted.append((inflow[r] * jnp.exp(final - run)).astype(BF16))
        sd[x, j] = jnp.broadcast_to(offset, sd.shape[2:])
    at_end(lambda: forward(2, 1))
    forward(2, 2)
    at_end(lambda: forward(2, 0))
    collect(1)
    both = dot(full, jnp.concatenate([weight(at_v), widen(gb[:, at_q:at_r])], axis=1)).astype(BF16)
    vals, queries = both[:, :w], both[:, w:]
    for j in (0, 1):
        carried = None
        for i in range(spans):
            r = slice(j * block + i * REC_SPAN, j * block + (i + 1) * REC_SPAN)
            final = running[j * spans + i][REC_SPAN - 1 : REC_SPAN]
            befores.append(carried)
            new = dot(vals[r], weighted[j * spans + i], TN)
            carried = new if carried is None else carried * jnp.exp(final) + new
        st[x, j] = carried.astype(BF16)
    st_swap(x).start()
    sd_swap(x).start()


    def advance(carried, sx, j):
        return carried * jnp.exp(sd[sx, j][0:1]) + st[sx, j].astype(F32)

    def un_pair(z2, owner):
        device = (4 * z2 + 2 * zl + x, t)
        return (
            remote(un.at[owner], un.at[owner], un_send.at[z2], un_recv.at[owner], device),
            remote(ud.at[owner], ud.at[owner], ud_send.at[z2], ud_recv.at[owner], device),
        )

    def un_start(z2):
        for copy in un_pair(z2, zh):
            copy.start()

    def un_wait(owner):
        for copy in un_pair(owner, owner):
            copy.wait_recv()

    def join_units():
        st_swap(1 - x).wait_recv()
        sd_swap(1 - x).wait_recv()
        unit = st[0, 0].astype(F32)
        for sx, j in ((1, 0), (0, 1), (1, 1)):
            unit = advance(unit, sx, j)
        un[zh] = unit.astype(BF16)
        ud[zh] = sd[0, 0] + sd[1, 0] + sd[0, 1] + sd[1, 1]
        loop(zh + 1, count_z, un_start)

    def un_done(z2):
        for copy in un_pair(z2, zh):
            copy.wait_send()

    keyvals.relay_y(1)
    keyvals.arrive()

    forward(3, 1)
    zs = max(1, min(count_z, KEY_BLOCK // (4 * block)))
    blocks = count_z // zs
    scale = math.log2(math.e) / math.sqrt(QK_DIM)

    def attend(query, b):
        both = kvb[:, :, :, pl.ds(b * zs, zs)].reshape(4 * zs * block, kvb.shape[5])
        values = both[:, 2 * QK_DIM :]
        parts = []
        for comp in range(2):
            cols = slice(comp * QK_DIM, (comp + 1) * QK_DIM)
            scores = dot(query[:, cols], both[:, cols], NT)
            peak = jnp.max(scores, axis=1, keepdims=True)
            expo = jnp.exp2((scores - peak) * scale)
            parts += [peak, jnp.sum(expo, axis=1, keepdims=True), dot(expo.astype(BF16), values)]
        return tuple(parts)

    def merge(a, b):
        parts = []
        for comp in range(2):
            pa, ta, wa = a[3 * comp : 3 * comp + 3]
            pc, tc, wc = b[3 * comp : 3 * comp + 3]
            peak = jnp.maximum(pa, pc)
            ea, ec = jnp.exp2((pa - peak) * scale), jnp.exp2((pc - peak) * scale)
            parts += [peak, ta * ea + tc * ec, wa * ea + wc * ec]
        return tuple(parts)

    hidden = []
    for j in (0, 1):
        query = queries[j * block : (j + 1) * block]
        got = attend(query, 0)
        if blocks > 1:
            got = lax.fori_loop(1, blocks, lambda b, g: merge(g, attend(query, b)), got)
        blended = got[2] / got[1] - mapw[zl] * (got[5] / got[4])
        hidden.append(rms(blended, again[...]))
    attn_hidden = jnp.concatenate(hidden, axis=0).astype(BF16)

    join_units()
    forward(3, 2)
    collect(2)
    raw = dot(full, weight(at_r)).astype(BF16).astype(F32)
    rec_query = raw * jax.nn.sigmoid(raw)
    local, lifted = [], []
    for j in (0, 1):
        outs, lifts = [], []
        for i in range(spans):
            r = slice(j * block + i * REC_SPAN, j * block + (i + 1) * REC_SPAN)
            run = running[j * spans + i]
            before = befores[j * spans + i]
            dq = (rec_query[r] * jnp.exp(run)).astype(BF16)
            within = dot(dq, (inflow[r] * jnp.exp(-run)).astype(BF16), NT) * lower
            o = dot(within.astype(BF16), vals[r])
            if before is not None:
                o = o + dot(dq, before.astype(BF16), NT)
            outs.append(o)
            lifts.append(rec_query[r] * jnp.exp(offsets[j * spans + i] + run))
        local.append(jnp.concatenate(outs, axis=0))
        lifted.append(jnp.concatenate(lifts, axis=0).astype(BF16))

    forward(3, 0)
    loop(0, zh, un_wait)

    def chain(k, carry):
        return carry * jnp.exp(ud[k][0:1]) + un[k].astype(F32)

    base = lax.fori_loop(0, zh, chain, init[zl].T)
    s01 = advance(base, 0, 0)
    s10 = advance(s01, 1, 0)
    s11 = advance(s10, 0, 1)
    incoming = (jnp.where(x == 0, base, s01), jnp.where(x == 0, s10, s11))
    rec = []
    for j in (0, 1):
        o = local[j] + dot(lifted[j], incoming[j].astype(BF16), NT)
        rec.append(rms(o, rgain[...]))
    rec_hidden = jnp.concatenate(rec, axis=0).astype(BF16)
    both_hidden = jnp.concatenate([rec_hidden, attn_hidden], axis=1)

    per = pb.shape[5] // part
    fw = per * part
    chunks = n // per

    def d_copy(ch):
        return remote(pb.at[ch, 1 - lo], db.at[ch], d_send.at[ch], d_recv.at[ch], (s, cmate))

    def y_copy(ch, k, flip):
        h2 = (hi + k) % count_h
        src = zb.at[ch, pl.ds(h2, 1)] if flip else sb.at[ch, pl.ds(2 * h2, 2)]
        dst = yr.at[ch, k, pl.ds(0, 1)] if flip else yr.at[ch, k]
        return remote(src, dst, y_send.at[ch, k], y_recv.at[ch, k], (s, 2 * h2 + lo))

    def z_copy(ch, flip):
        src = sb.at[ch, pl.ds(count_h * (1 - zl), count_h)] if flip else zb.at[ch, pl.ds(1 - zl, 1)]
        dst = zr.at[ch] if flip else zr.at[ch, pl.ds(0, 1)]
        return remote(src, dst, z_send.at[ch], z_recv.at[ch], (zmate, t))

    def stage_d(ch):
        shard = gb[pl.ds(ch * per, per)]
        weights = jnp.concatenate(
            [shard[:, at_o:].reshape(fw, w), widen(shard[:, at_a:at_o])], axis=1
        )
        got = dot(both_hidden, weights, NT).astype(BF16)
        for z2 in (0, 1):
            for t2 in range(nt):
                lo_row = (z2 * nt + t2) * rows
                pb[ch, t2 % 2, z2, t2 // 2] = got[lo_row : lo_row + rows]
        d_copy(ch).start()

    def stage_first(ch, flip):
        d_copy(ch).wait_recv()
        total = (pb[ch, lo].astype(F32) + db[ch].astype(F32)).astype(BF16)
        if flip:
            sb[ch] = total.reshape(sb.shape[1:])
            z_copy(ch, flip).start()
        else:
            for h2 in range(count_h):
                sb[ch, 2 * h2 : 2 * h2 + 2] = total[:, h2]
            for k in range(1, count_h):
                y_copy(ch, k, flip).start()

    def stage_second(ch, flip):
        if flip:
            z_copy(ch, flip).wait_recv()
            mine = sb[ch, pl.ds(count_h * zl, count_h)]
            zb[ch] = (mine.astype(F32) + zr[ch].astype(F32)).astype(BF16)
            for k in range(1, count_h):
                y_copy(ch, k, flip).start()
        else:
            total = sb[ch, pl.ds(2 * hi, 2)].astype(F32)
            for k in range(1, count_h):
                y_copy(ch, k, flip).wait_recv()
                total = total + yr[ch, k].astype(F32)
            zb[ch, 0:2] = total.astype(BF16)
            z_copy(ch, flip).start()

    def stage_out(ch, flip):
        if flip:
            total = zb[ch, hi].astype(F32)
            for k in range(1, count_h):
                y_copy(ch, k, flip).wait_recv()
                total = total + yr[ch, k, 0].astype(F32)
        else:
            z_copy(ch, flip).wait_recv()
            total = zb[ch, zl].astype(F32) + zr[ch, 0].astype(F32)
        out[:, pl.ds(pl.multiple_of(ch * fw, fw), fw)] = total.astype(out.dtype)
        store(ch).start()

    def store(ch):
        cols = pl.ds(pl.multiple_of(ch * fw, fw), fw)
        return pltpu.make_async_copy(out.at[:, cols], out_ref.at[:, cols], out_sem.at[ch])

    if small and per == 1:
        order = [(q, c) for c in (0, 1) for q in (2 * zh, 2 * zh + 1)]
        order += [(q, c) for q in (sources[2], sources[0]) for c in (0, 1)]
        ready = []
        for q, c in order:
            ready.append((2 * q + x if c == 0 else 2 * q + 1 - x, q if c == 1 else None))
    else:
        collect(3)
        ready = [(ch, None) for ch in range(chunks)]

    lag = len(ready)
    for i in range(lag + LAGS[2]):
        if i < lag:
            ch, q = ready[i]
            if q is not None:
                row_in(q, 3).wait_recv()
            stage_d(ch)
        for body, late in zip((stage_first, stage_second, stage_out), LAGS):
            if 0 <= i - late < lag:
                body(ready[i - late][0], (i - late) % 2 == 1)

    for g in (0, 1, 2, 3):
        finish(g)
    tokens.finish()
    keyvals.finish()
    loop(1, count_z, lambda j: k1_copy(j, zh).wait_send())
    kv_swap(x).wait_send()
    extra_swap().wait_send()
    st_swap(x).wait_send()
    sd_swap(x).wait_send()
    loop(zh + 1, count_z, un_done)

    for i, (ch, _) in enumerate(ready):
        d_copy(ch).wait_send()
        for k in range(1, count_h):
            y_copy(ch, k, i % 2 == 1).wait_send()
        z_copy(ch, i % 2 == 1).wait_send()
        store(ch).wait()


def solution(mesh):
    n, nt = mesh.shape["sp"], mesh.shape["tp"]

    def body(
        tokens, input_norm_gain, paired_query_weight, shared_key_weight, shared_value_weight,
        recurrent_query_weight, forget_gate_weight, recurrent_value_weight,
        attention_output_weight, recurrent_output_weight, attention_head_gain,
        recurrent_head_gain, second_map_weight, forget_leak_rate, extra_log_decay,
        initial_recurrent_state,
    ):
        rows, width = tokens.shape
        weights = (
            paired_query_weight, forget_gate_weight, recurrent_value_weight,
            recurrent_query_weight, attention_output_weight, recurrent_output_weight,
        )
        part = forget_gate_weight.shape[0]
        span = extra_log_decay.shape[0]
        count_p, count_z, count_h = n // 2, n // 4, nt // 2
        fw = part * max(1, OUT_WIDTH // part)
        chunks = width // fw
        kv_width = 2 * QK_DIM + HEAD_DIM
        wk, wval = shared_key_weight.T, shared_value_weight.T
        staged = (tokens, *weights, wk, wval, extra_log_decay, initial_recurrent_state)
        hb = pl.BlockSpec(memory_space=pl.ANY)
        vm = pl.BlockSpec(memory_space=pltpu.VMEM)
        sm = pl.BlockSpec(memory_space=pltpu.SMEM)
        dma = pltpu.SemaphoreType.DMA
        w = RECURRENT_WIDTH
        return pl.pallas_call(
            functools.partial(kernel, n, nt),
            out_shape=jax.ShapeDtypeStruct((rows, width), BF16),
            in_specs=[hb, vm] + [hb] * 8 + [vm] * 2 + [sm, vm, hb, hb],
            out_specs=hb,
            scratch_shapes=[pltpu.VMEM(a.shape, a.dtype) for a in staged] + [
                pltpu.VMEM((rows, width), BF16),
                dma((len(staged),)), dma((chunks,)),
                pltpu.VMEM((n, 5 * part, w), BF16),
                pltpu.VMEM((5 * part, w), BF16),
                pltpu.VMEM((2, nt, rows, width), BF16),
                pltpu.VMEM((2, nt, 2, count_z, rows, kv_width), BF16),
                pltpu.VMEM((span, w), BF16),
                pltpu.VMEM((span, w), BF16),
                pltpu.VMEM((2, 2, w, w), BF16),
                pltpu.VMEM((2, 2, 8, w), F32),
                pltpu.VMEM((count_z, w, w), BF16),
                pltpu.VMEM((count_z, 8, w), F32),
                pltpu.VMEM((chunks, 2, 2, count_h, rows, fw), BF16),
                pltpu.VMEM((chunks, 2, count_h, rows, fw), BF16),
                pltpu.VMEM((chunks, 2 * count_h, rows, fw), BF16),
                pltpu.VMEM((chunks, count_h, 2, rows, fw), BF16),
                pltpu.VMEM((chunks, max(2, count_h), rows, fw), BF16),
                pltpu.VMEM((chunks, max(2, count_h), rows, fw), BF16),
                dma((count_p, 4)), dma((count_p, 4)),
                dma((count_p, 4)), dma((count_p, 4)),
                dma((3, 2, count_h)), dma((3, 2, count_h)),
                dma((3, 2, count_h)), dma((3, 2, count_h)),
                dma((count_z,)), dma((count_z,)),
                dma((4,)), dma((4,)),
                dma((count_z,)), dma((count_z,)),
                dma((count_z,)), dma((count_z,)),
                dma((chunks,)), dma((chunks,)),
                dma((chunks, count_h)), dma((chunks, count_h)),
                dma((chunks,)), dma((chunks,)),
            ],
            compiler_params=pltpu.CompilerParams(
                has_side_effects=True, collective_id=0, vmem_limit_bytes=60 * 1024 * 1024
            ),
        )(
            tokens, input_norm_gain[None], *weights, wk, wval,
            attention_head_gain[None], recurrent_head_gain[None], second_map_weight,
            forget_leak_rate[None], extra_log_decay, initial_recurrent_state,
        )

    placed = (
        P(("sp", "tp"), None), P(), P("sp", "tp"), P(), P(), P("sp", "tp"), P("sp", "tp"),
        P("sp", "tp"), P("sp", "tp"), P("sp", "tp"), P(), P(), P("tp"), P("tp"),
        P("sp", "tp"), P("tp", None, None),
    )
    return jax.shard_map(
        body, mesh=mesh, in_specs=placed, out_specs=P(("sp", "tp"), None), check_vma=False
    )
```

```python
import functools
import math

import jax
import jax.numpy as jnp
from jax import lax
from jax.experimental import pallas as pl
from jax.experimental.pallas import tpu as pltpu
from jax.sharding import PartitionSpec as P

QK_DIM = 32
HEAD_DIM = 64
RECURRENT_WIDTH = 128
REC_SPAN = 64
KEY_BLOCK = 1536
OUT_WIDTH = 256
LAGS = (2, 8, 14)
EPS = 1e-06
MESH = pl.DeviceIdType.MESH
F32, BF16 = jnp.float32, jnp.bfloat16

NN = (((1,), (0,)), ((), ()))
NT = (((1,), (1,)), ((), ()))
TN = (((0,), (0,)), ((), ()))


def dot(a, b, dims=NN, precision=None):
    return lax.dot_general(a, b, dims, preferred_element_type=F32, precision=precision)


def rms(x, gain):
    return x * lax.rsqrt(jnp.mean(x * x, axis=-1, keepdims=True) + EPS) * gain


def loop(lo, hi, body):
    def step(j, carry):
        body(j)
        return carry

    lax.fori_loop(lo, hi, step, 0)


def kernel(
    n, nt,
    tok_in, gain, wq_in, wg_in, wv_in, wr_in, woa_in, wor_in, wk_in, wval_in, again, rgain, mapw, leak,
    extra_in, init_in,
    out_ref,
    tok, wq, wg, wv, wr, woa, wor, wk, wval, extra, init, out, in_sem, out_sem,
    gb, pk, nf, kvb, xb, xs, st, sd, un, ud, pb, db, sb, yr, zb, zr,
    col_send, col_recv, row_send, row_recv, tg_send, tg_recv, kg_send, kg_recv,
    k1_send, k1_recv, x_send, x_recv, un_send, un_recv, ud_send, ud_recv,
    d_send, d_recv, y_send, y_recv, z_send, z_recv,
):
    s, t = lax.axis_index("sp"), lax.axis_index("tp")
    count_p, count_z, count_h = n // 2, n // 4, nt // 2
    small = count_p <= 4
    x, p = s % 2, s // 2
    zl, zh = p % 2, p // 2
    hi, lo = t // 2, t % 2
    zmate, xmate, cmate = s + 2 - 4 * zl, s + 1 - 2 * x, t + 1 - 2 * lo

    def remote(src, dst, send_sem, recv_sem, device):
        return pltpu.make_async_remote_copy(
            src_ref=src, dst_ref=dst, send_sem=send_sem, recv_sem=recv_sem,
            device_id=device, device_id_type=MESH,
        )

    order_in = (
        (wg_in, wg), (tok_in, tok), (wk_in, wk), (wval_in, wval), (wv_in, wv), (wq_in, wq),
        (extra_in, extra), (wr_in, wr), (woa_in, woa), (wor_in, wor), (init_in, init),
    )
    loads = [pltpu.make_async_copy(a, b, in_sem.at[i]) for i, (a, b) in enumerate(order_in)]
    for load in loads:
        load.start()
    barrier = pltpu.get_barrier_semaphore()

    def greet(peer):
        pl.semaphore_signal(barrier, inc=1, device_id=peer, device_id_type=MESH)

    loop(1, count_p, lambda j: greet((2 * ((p + j) % count_p) + x, t)))
    greet((xmate, t))
    greet((s, cmate))
    for k in range(1, count_h):
        greet((s, (t + 2 * k) % nt))

    def need(*refs):
        for load, (_, b) in zip(loads, order_in):
            if any(b is r for r in refs):
                load.wait()

    rows, width = tok.shape
    part, half, w = wg.shape[0], wg.shape[0] // 2, RECURRENT_WIDTH
    at_v, at_q, at_r, at_a, at_o = part, 2 * part, 2 * part + half, 3 * part + half, 4 * part
    groups = ((0, at_v), (at_v, at_r), (at_r, at_a), (at_a, 5 * part))

    def split(ref, lo_row):
        mine = pl.ds(pl.multiple_of(zl * w, w), w)
        other = pl.ds(pl.multiple_of((1 - zl) * w, w), w)
        gb[s, lo_row : lo_row + part] = ref[:, mine]
        pk[lo_row : lo_row + part] = ref[:, other]

    def split_narrow(ref, lo_row):
        v = ref[...]
        a = v.shape[1] // 2
        first = jnp.concatenate([v[:half, :a], v[half:, :a]], axis=1)
        second = jnp.concatenate([v[:half, a:], v[half:, a:]], axis=1)
        gb[s, lo_row : lo_row + half] = jnp.where(zl == 0, first, second)
        pk[lo_row : lo_row + half] = jnp.where(zl == 0, second, first)

    class Gather:
        def __init__(self, ref, send, recv):
            self.ref, self.send, self.recv = ref, send, recv

        def slot(self, zz, owner):
            return self.ref.at[zl if zz == 0 else 1 - zl, owner % nt]

        def copy(self, kind, zz, k, owner, device):
            block = self.slot(zz, owner)
            return remote(block, block, self.send.at[kind, zz, k], self.recv.at[kind, zz, k], device)

        def core_out(self, zz, k):
            return self.copy(0, zz, k, t + nt - 2 * k, (s, cmate))

        def core_in(self, zz, k):
            return self.copy(0, zz, k, cmate + nt - 2 * k, (s, cmate))

        def y_out(self, zz, k):
            return self.copy(1, zz, k, t, (s, (t + 2 * k) % nt))

        def y_in(self, zz, k):
            return self.copy(1, zz, k, t + nt - 2 * k, (s, (t + nt - 2 * k) % nt))

        def z_out(self):
            return self.copy(2, 0, 0, t, (zmate, t))

        def z_in(self):
            block = self.slot(1, t)
            return remote(block, block, self.send.at[2, 0, 0], self.recv.at[2, 0, 0], (zmate, t))

        def start(self):
            self.z_out().start()
            for k in range(1, count_h):
                self.y_out(0, k).start()
            self.core_out(0, 0).start()

        def relay_z(self):
            self.z_in().wait_recv()
            for k in range(1, count_h):
                self.y_out(1, k).start()
            self.core_out(1, 0).start()

        def relay_y(self, zz):
            for k in range(1, count_h):
                self.y_in(zz, k).wait_recv()
                self.core_out(zz, k).start()

        def arrive(self):
            for zz in (0, 1):
                for k in range(count_h):
                    self.core_in(zz, k).wait_recv()

        def finish(self):
            self.z_out().wait_send()
            for zz in (0, 1):
                for k in range(count_h):
                    self.core_out(zz, k).wait_send()
                    if k > 0:
                        self.y_out(zz, k).wait_send()

    tokens, keyvals = Gather(nf, tg_send, tg_recv), Gather(kvb, kg_send, kg_recv)

    def cut(ref, g):
        return ref.at[groups[g][0] : groups[g][1]]

    def col_out(p2, g, same):
        return remote(
            cut(gb.at[s], g) if same else cut(pk, g), cut(gb.at[s], g),
            col_send.at[p2, g], col_recv.at[p, g], (2 * p2 + x, t),
        )

    def col_in(p2, g):
        slot = cut(gb.at[2 * p2 + x], g)
        return remote(slot, slot, col_send.at[p2, g], col_recv.at[p2, g], (2 * p2 + x, t))

    def row_out(p2, g):
        slot = cut(gb.at[2 * p2 + x], g)
        return remote(slot, slot, row_send.at[p2, g], row_recv.at[p2, g], (xmate, t))

    def row_in(p2, g):
        slot = cut(gb.at[2 * p2 + 1 - x], g)
        return remote(slot, slot, row_send.at[p2, g], row_recv.at[p2, g], (xmate, t))

    def near(d, body):
        for sign in (1, -1):
            p2 = p + sign * d

            @pl.when((p2 >= 0) & (p2 < count_p))
            def _():
                body(p2)

    def distances(body):
        if small:
            for d in range(1, count_p):
                body(d, d % 2 == 0)
        else:
            loop(0, count_p // 2, lambda i: body(2 * i + 1, False))
            loop(1, count_p // 2, lambda i: body(2 * i, True))

    def columns(g):
        distances(lambda d, same: near(d, lambda p2: col_out(p2, g, same).start()))

    sources = (count_z - zh, p + 1 - 2 * zl, (count_p - 1) * (1 - zh))

    def forward_one(g, p2):
        col_in(p2, g).wait_recv()
        row_out(p2, g).start()

    def forward(g, i):
        if small:
            forward_one(g, sources[i])
        elif i == 0:
            loop(1, count_p, lambda e: near(e, lambda p2: forward_one(g, p2)))

    at_edge = (p == 0) | (p == count_p - 1)

    def at_end(body):
        if small:
            pl.when(at_edge)(body)

    def at_middle(body):
        if small:
            pl.when(jnp.logical_not(at_edge))(body)
        else:
            body()

    def collect(g):
        loop(0, count_p, lambda p2: row_in(p2, g).wait_recv())

    def finish(g):
        distances(lambda d, same: near(d, lambda p2: col_out(p2, g, same).wait_send()))
        loop(0, count_p, lambda p2: row_out(p2, g).wait_send())

    def k1_copy(j, owner):
        block = kvb.at[zl, t, x, owner % count_z]
        peer = (zh + j) % count_z
        return remote(block, block, k1_send.at[j], k1_recv.at[j], (4 * peer + 2 * zl + x, t))

    def swap(i, src, dst, device):
        return remote(src, dst, x_send.at[i], x_recv.at[i], device)

    def kv_swap(side):
        return swap(0, kvb.at[zl, t, side], kvb.at[zl, t, side], (xmate, t))

    def extra_swap():
        return swap(1, xs, xb, (zmate, t))

    def st_swap(side):
        return swap(2, st.at[side], st.at[side], (xmate, t))

    def sd_swap(side):
        return swap(3, sd.at[side], sd.at[side], (xmate, t))

    need(wg)
    split(wg, 0)
    pl.semaphore_wait(barrier, count_p + count_h)
    row_out(p, 0).start()
    columns(0)
    need(tok)
    normed = rms(tok[...].astype(F32), gain[...]).astype(BF16)
    nf[zl, t] = normed
    need(wk, wval)
    kvb[zl, t, x, zh] = jnp.concatenate(
        [dot(normed, wk[...], NT).astype(BF16), dot(normed, wval[...], NT).astype(BF16)], axis=1
    )
    loop(1, count_z, lambda j: k1_copy(j, zh).start())
    tokens.start()
    need(wv, wq)
    split(wv, at_v)
    split_narrow(wq, at_q)
    row_out(p, 1).start()
    columns(1)
    need(extra)
    xs[...] = extra[:, pl.ds(pl.multiple_of((1 - zl) * w, w), w)].astype(BF16)
    extra_swap().start()
    need(wr, woa, wor, init)
    split(wr, at_r)
    split_narrow(woa, at_a)
    split(wor, at_o)
    forward(0, 1)
    forward(0, 0)
    forward(0, 2)
    loop(1, count_z, lambda j: k1_copy(j, zh + count_z - j).wait_recv())
    kv_swap(x).start()
    row_out(p, 2).start()
    row_out(p, 3).start()
    tokens.relay_y(0)
    at_middle(lambda: forward(1, 0))
    kv_swap(1 - x).wait_recv()
    keyvals.start()
    columns(2)
    tokens.relay_z()
    forward(1, 1)
    at_end(lambda: forward(1, 0))
    tokens.relay_y(1)
    forward(1, 2)
    columns(3)
    keyvals.relay_z()
    keyvals.relay_y(0)
    at_middle(lambda: forward(2, 0))
    at_middle(lambda: forward(2, 1))
    tokens.arrive()
    extra_swap().wait_recv()
    collect(0)

    block = nt * rows
    full = nf[...].reshape(2 * block, width)

    def weight(lo_row):
        return gb[:, lo_row : lo_row + part].reshape(n * part, w)

    def widen(v):
        a = v.shape[2] // 2
        both = jnp.concatenate([v[:, :, :a], v[:, :, a:]], axis=1)
        return both.reshape(both.shape[0] * both.shape[1], a)

    gate = dot(full, weight(0)).astype(BF16).astype(F32)
    leak_mine = jnp.where(zl == 0, leak[:, :w], leak[:, w:])
    inflow = leak_mine * (1.0 - jax.nn.sigmoid(gate))
    here = extra[:, pl.ds(pl.multiple_of(zl * w, w), w)]
    there = xb[...].astype(F32)
    added = jnp.concatenate([jnp.where(zl == 0, here, there), jnp.where(zl == 0, there, here)], axis=0)
    log_decay = jnp.log(1.0 - inflow) + added
    spans = block // REC_SPAN
    rr = lax.broadcasted_iota(jnp.int32, (REC_SPAN, REC_SPAN), 0)
    cc = lax.broadcasted_iota(jnp.int32, (REC_SPAN, REC_SPAN), 1)
    lower = (rr >= cc).astype(F32)
    running, offsets, befores, weighted, grown, shrunk = [], [], [], [], [], []
    for j in (0, 1):
        offset = jnp.zeros((1, w), F32)
        for i in range(spans):
            r = slice(j * block + i * REC_SPAN, j * block + (i + 1) * REC_SPAN)
            run = dot(lower, log_decay[r], precision=lax.Precision.HIGHEST)
            final = run[REC_SPAN - 1 : REC_SPAN]
            running.append(run)
            offsets.append(offset)
            offset = offset + final
            weighted.append((inflow[r] * jnp.exp(final - run)).astype(BF16))
            grown.append(jnp.exp(run))
            shrunk.append((inflow[r] * jnp.exp(-run)).astype(BF16))
        sd[x, j] = jnp.broadcast_to(offset, sd.shape[2:])
    at_end(lambda: forward(2, 1))
    forward(2, 2)
    at_end(lambda: forward(2, 0))
    collect(1)
    both = dot(full, jnp.concatenate([weight(at_v), widen(gb[:, at_q:at_r])], axis=1)).astype(BF16)
    vals, queries = both[:, :w], both[:, w:]
    for j in (0, 1):
        carried = None
        for i in range(spans):
            r = slice(j * block + i * REC_SPAN, j * block + (i + 1) * REC_SPAN)
            final = running[j * spans + i][REC_SPAN - 1 : REC_SPAN]
            befores.append(carried)
            new = dot(vals[r], weighted[j * spans + i], TN)
            carried = new if carried is None else carried * jnp.exp(final) + new
        st[x, j] = carried.astype(BF16)
    st_swap(x).start()
    sd_swap(x).start()


    def advance(carried, sx, j):
        return carried * jnp.exp(sd[sx, j][0:1]) + st[sx, j].astype(F32)

    def un_pair(z2, owner):
        device = (4 * z2 + 2 * zl + x, t)
        return (
            remote(un.at[owner], un.at[owner], un_send.at[z2], un_recv.at[owner], device),
            remote(ud.at[owner], ud.at[owner], ud_send.at[z2], ud_recv.at[owner], device),
        )

    def un_start(z2):
        for copy in un_pair(z2, zh):
            copy.start()

    def un_wait(owner):
        for copy in un_pair(owner, owner):
            copy.wait_recv()

    def join_units():
        st_swap(1 - x).wait_recv()
        sd_swap(1 - x).wait_recv()
        unit = st[0, 0].astype(F32)
        for sx, j in ((1, 0), (0, 1), (1, 1)):
            unit = advance(unit, sx, j)
        un[zh] = unit.astype(BF16)
        ud[zh] = sd[0, 0] + sd[1, 0] + sd[0, 1] + sd[1, 1]
        loop(zh + 1, count_z, un_start)

    def un_done(z2):
        for copy in un_pair(z2, zh):
            copy.wait_send()

    keyvals.relay_y(1)
    keyvals.arrive()

    forward(3, 1)
    zs = max(1, min(count_z, KEY_BLOCK // (4 * block)))
    blocks = count_z // zs
    scale = math.log2(math.e) / math.sqrt(QK_DIM)

    def attend(query, b):
        both = kvb[:, :, :, pl.ds(b * zs, zs)].reshape(4 * zs * block, kvb.shape[5])
        values = both[:, 2 * QK_DIM :]
        parts = []
        for comp in range(2):
            cols = slice(comp * QK_DIM, (comp + 1) * QK_DIM)
            scores = dot(query[:, cols], both[:, cols], NT)
            peak = jnp.max(scores, axis=1, keepdims=True)
            expo = jnp.exp2((scores - peak) * scale)
            parts += [peak, jnp.sum(expo, axis=1, keepdims=True), dot(expo.astype(BF16), values)]
        return tuple(parts)

    def merge(a, b):
        parts = []
        for comp in range(2):
            pa, ta, wa = a[3 * comp : 3 * comp + 3]
            pc, tc, wc = b[3 * comp : 3 * comp + 3]
            peak = jnp.maximum(pa, pc)
            ea, ec = jnp.exp2((pa - peak) * scale), jnp.exp2((pc - peak) * scale)
            parts += [peak, ta * ea + tc * ec, wa * ea + wc * ec]
        return tuple(parts)

    hidden = []
    for j in (0, 1):
        query = queries[j * block : (j + 1) * block]
        got = attend(query, 0)
        if blocks > 1:
            got = lax.fori_loop(1, blocks, lambda b, g: merge(g, attend(query, b)), got)
        blended = got[2] / got[1] - mapw[zl] * (got[5] / got[4])
        hidden.append(rms(blended, again[...]))
    attn_hidden = jnp.concatenate(hidden, axis=0).astype(BF16)

    def raw_term(owner):
        rows_in = nf[:, :, :, pl.ds(pl.multiple_of(owner * part, part), part)]
        return dot(rows_in.reshape(2 * block, part), gb[owner, at_r:at_a])

    stepwise = small and part % 128 == 0
    pieces = (p, sources[1], sources[2], sources[0])
    if stepwise:
        raw = raw_term(2 * pieces[0] + x)
        for q in pieces[1:]:
            raw = raw + raw_term(2 * q + x)
    join_units()
    forward(3, 2)
    if stepwise:
        for q in pieces:
            row_in(q, 2).wait_recv()
            raw = raw + raw_term(2 * q + 1 - x)
    else:
        collect(2)
        raw = dot(full, weight(at_r))
    raw = raw.astype(BF16).astype(F32)
    rec_query = raw * jax.nn.sigmoid(raw)
    local, lifted = [], []
    for j in (0, 1):
        outs, lifts = [], []
        for i in range(spans):
            r = slice(j * block + i * REC_SPAN, j * block + (i + 1) * REC_SPAN)
            m = j * spans + i
            decayed = rec_query[r] * grown[m]
            dq = decayed.astype(BF16)
            within = dot(dq, shrunk[m], NT) * lower
            o = dot(within.astype(BF16), vals[r])
            if befores[m] is not None:
                o = o + dot(dq, befores[m].astype(BF16), NT)
            outs.append(o)
            lifts.append(decayed * jnp.exp(offsets[m]))
        local.append(jnp.concatenate(outs, axis=0))
        lifted.append(jnp.concatenate(lifts, axis=0).astype(BF16))

    forward(3, 0)
    loop(0, zh, un_wait)

    def chain(k, carry):
        return carry * jnp.exp(ud[k][0:1]) + un[k].astype(F32)

    base = lax.fori_loop(0, zh, chain, init[zl].T)
    s01 = advance(base, 0, 0)
    s10 = advance(s01, 1, 0)
    s11 = advance(s10, 0, 1)
    incoming = (jnp.where(x == 0, base, s01), jnp.where(x == 0, s10, s11))
    rec = []
    for j in (0, 1):
        o = local[j] + dot(lifted[j], incoming[j].astype(BF16), NT)
        rec.append(rms(o, rgain[...]))
    rec_hidden = jnp.concatenate(rec, axis=0).astype(BF16)
    both_hidden = jnp.concatenate([rec_hidden, attn_hidden], axis=1)

    per = pb.shape[5] // part
    fw = per * part
    chunks = n // per

    def d_copy(ch):
        return remote(pb.at[ch, 1 - lo], db.at[ch], d_send.at[ch], d_recv.at[ch], (s, cmate))

    def y_copy(ch, k, flip):
        h2 = (hi + k) % count_h
        src = zb.at[ch, pl.ds(h2, 1)] if flip else sb.at[ch, pl.ds(2 * h2, 2)]
        dst = yr.at[ch, k, pl.ds(0, 1)] if flip else yr.at[ch, k]
        return remote(src, dst, y_send.at[ch, k], y_recv.at[ch, k], (s, 2 * h2 + lo))

    def z_copy(ch, flip):
        src = sb.at[ch, pl.ds(count_h * (1 - zl), count_h)] if flip else zb.at[ch, pl.ds(1 - zl, 1)]
        dst = zr.at[ch] if flip else zr.at[ch, pl.ds(0, 1)]
        return remote(src, dst, z_send.at[ch], z_recv.at[ch], (zmate, t))

    def stage_d(ch):
        shard = gb[pl.ds(ch * per, per)]
        weights = jnp.concatenate(
            [shard[:, at_o:].reshape(fw, w), widen(shard[:, at_a:at_o])], axis=1
        )
        got = dot(both_hidden, weights, NT).astype(BF16)
        for z2 in (0, 1):
            for t2 in range(nt):
                lo_row = (z2 * nt + t2) * rows
                pb[ch, t2 % 2, z2, t2 // 2] = got[lo_row : lo_row + rows]
        d_copy(ch).start()

    def stage_first(ch, flip):
        d_copy(ch).wait_recv()
        total = (pb[ch, lo].astype(F32) + db[ch].astype(F32)).astype(BF16)
        if flip:
            sb[ch] = total.reshape(sb.shape[1:])
            z_copy(ch, flip).start()
        else:
            for h2 in range(count_h):
                sb[ch, 2 * h2 : 2 * h2 + 2] = total[:, h2]
            for k in range(1, count_h):
                y_copy(ch, k, flip).start()

    def stage_second(ch, flip):
        if flip:
            z_copy(ch, flip).wait_recv()
            mine = sb[ch, pl.ds(count_h * zl, count_h)]
            zb[ch] = (mine.astype(F32) + zr[ch].astype(F32)).astype(BF16)
            for k in range(1, count_h):
                y_copy(ch, k, flip).start()
        else:
            total = sb[ch, pl.ds(2 * hi, 2)].astype(F32)
            for k in range(1, count_h):
                y_copy(ch, k, flip).wait_recv()
                total = total + yr[ch, k].astype(F32)
            zb[ch, 0:2] = total.astype(BF16)
            z_copy(ch, flip).start()

    def stage_out(ch, flip):
        if flip:
            total = zb[ch, hi].astype(F32)
            for k in range(1, count_h):
                y_copy(ch, k, flip).wait_recv()
                total = total + yr[ch, k, 0].astype(F32)
        else:
            z_copy(ch, flip).wait_recv()
            total = zb[ch, zl].astype(F32) + zr[ch, 0].astype(F32)
        out[:, pl.ds(pl.multiple_of(ch * fw, fw), fw)] = total.astype(out.dtype)
        store(ch).start()

    def store(ch):
        cols = pl.ds(pl.multiple_of(ch * fw, fw), fw)
        return pltpu.make_async_copy(out.at[:, cols], out_ref.at[:, cols], out_sem.at[ch])

    if small and per == 1:
        order = [(q, c) for c in (0, 1) for q in (2 * zh, 2 * zh + 1)]
        order += [(q, c) for q in (sources[2], sources[0]) for c in (0, 1)]
        ready = []
        for q, c in order:
            ready.append((2 * q + x if c == 0 else 2 * q + 1 - x, q if c == 1 else None))
    else:
        collect(3)
        ready = [(ch, None) for ch in range(chunks)]

    lag = len(ready)
    for i in range(lag + LAGS[2]):
        if i < lag:
            ch, q = ready[i]
            if q is not None:
                row_in(q, 3).wait_recv()
            stage_d(ch)
        for body, late in zip((stage_first, stage_second, stage_out), LAGS):
            if 0 <= i - late < lag:
                body(ready[i - late][0], (i - late) % 2 == 1)

    for g in (0, 1, 2, 3):
        finish(g)
    tokens.finish()
    keyvals.finish()
    loop(1, count_z, lambda j: k1_copy(j, zh).wait_send())
    kv_swap(x).wait_send()
    extra_swap().wait_send()
    st_swap(x).wait_send()
    sd_swap(x).wait_send()
    loop(zh + 1, count_z, un_done)

    for i, (ch, _) in enumerate(ready):
        d_copy(ch).wait_send()
        for k in range(1, count_h):
            y_copy(ch, k, i % 2 == 1).wait_send()
        z_copy(ch, i % 2 == 1).wait_send()
        store(ch).wait()


def solution(mesh):
    n, nt = mesh.shape["sp"], mesh.shape["tp"]

    def body(
        tokens, input_norm_gain, paired_query_weight, shared_key_weight, shared_value_weight,
        recurrent_query_weight, forget_gate_weight, recurrent_value_weight,
        attention_output_weight, recurrent_output_weight, attention_head_gain,
        recurrent_head_gain, second_map_weight, forget_leak_rate, extra_log_decay,
        initial_recurrent_state,
    ):
        rows, width = tokens.shape
        weights = (
            paired_query_weight, forget_gate_weight, recurrent_value_weight,
            recurrent_query_weight, attention_output_weight, recurrent_output_weight,
        )
        part = forget_gate_weight.shape[0]
        span = extra_log_decay.shape[0]
        count_p, count_z, count_h = n // 2, n // 4, nt // 2
        fw = part * max(1, OUT_WIDTH // part)
        chunks = width // fw
        kv_width = 2 * QK_DIM + HEAD_DIM
        wk, wval = shared_key_weight.T, shared_value_weight.T
        staged = (tokens, *weights, wk, wval, extra_log_decay, initial_recurrent_state)
        hb = pl.BlockSpec(memory_space=pl.ANY)
        vm = pl.BlockSpec(memory_space=pltpu.VMEM)
        sm = pl.BlockSpec(memory_space=pltpu.SMEM)
        dma = pltpu.SemaphoreType.DMA
        w = RECURRENT_WIDTH
        return pl.pallas_call(
            functools.partial(kernel, n, nt),
            out_shape=jax.ShapeDtypeStruct((rows, width), BF16),
            in_specs=[hb, vm] + [hb] * 8 + [vm] * 2 + [sm, vm, hb, hb],
            out_specs=hb,
            scratch_shapes=[pltpu.VMEM(a.shape, a.dtype) for a in staged] + [
                pltpu.VMEM((rows, width), BF16),
                dma((len(staged),)), dma((chunks,)),
                pltpu.VMEM((n, 5 * part, w), BF16),
                pltpu.VMEM((5 * part, w), BF16),
                pltpu.VMEM((2, nt, rows, width), BF16),
                pltpu.VMEM((2, nt, 2, count_z, rows, kv_width), BF16),
                pltpu.VMEM((span, w), BF16),
                pltpu.VMEM((span, w), BF16),
                pltpu.VMEM((2, 2, w, w), BF16),
                pltpu.VMEM((2, 2, 8, w), F32),
                pltpu.VMEM((count_z, w, w), BF16),
                pltpu.VMEM((count_z, 8, w), F32),
                pltpu.VMEM((chunks, 2, 2, count_h, rows, fw), BF16),
                pltpu.VMEM((chunks, 2, count_h, rows, fw), BF16),
                pltpu.VMEM((chunks, 2 * count_h, rows, fw), BF16),
                pltpu.VMEM((chunks, count_h, 2, rows, fw), BF16),
                pltpu.VMEM((chunks, max(2, count_h), rows, fw), BF16),
                pltpu.VMEM((chunks, max(2, count_h), rows, fw), BF16),
                dma((count_p, 4)), dma((count_p, 4)),
                dma((count_p, 4)), dma((count_p, 4)),
                dma((3, 2, count_h)), dma((3, 2, count_h)),
                dma((3, 2, count_h)), dma((3, 2, count_h)),
                dma((count_z,)), dma((count_z,)),
                dma((4,)), dma((4,)),
                dma((count_z,)), dma((count_z,)),
                dma((count_z,)), dma((count_z,)),
                dma((chunks,)), dma((chunks,)),
                dma((chunks, count_h)), dma((chunks, count_h)),
                dma((chunks,)), dma((chunks,)),
            ],
            compiler_params=pltpu.CompilerParams(
                has_side_effects=True, collective_id=0, vmem_limit_bytes=60 * 1024 * 1024
            ),
        )(
            tokens, input_norm_gain[None], *weights, wk, wval,
            attention_head_gain[None], recurrent_head_gain[None], second_map_weight,
            forget_leak_rate[None], extra_log_decay, initial_recurrent_state,
        )

    placed = (
        P(("sp", "tp"), None), P(), P("sp", "tp"), P(), P(), P("sp", "tp"), P("sp", "tp"),
        P("sp", "tp"), P("sp", "tp"), P("sp", "tp"), P(), P(), P("tp"), P("tp"),
        P("sp", "tp"), P("tp", None, None),
    )
    return jax.shard_map(
        body, mesh=mesh, in_specs=placed, out_specs=P(("sp", "tp"), None), check_vma=False
    )
```

```python
import functools
import math

import jax
import jax.numpy as jnp
from jax import lax
from jax.experimental import pallas as pl
from jax.experimental.pallas import tpu as pltpu
from jax.sharding import PartitionSpec as P

QK_DIM = 32
HEAD_DIM = 64
RECURRENT_WIDTH = 128
REC_SPAN = 64
KEY_BLOCK = 1536
OUT_WIDTH = 256
LAGS = (2, 8, 14)
EPS = 1e-06
MESH = pl.DeviceIdType.MESH
F32, BF16 = jnp.float32, jnp.bfloat16

NN = (((1,), (0,)), ((), ()))
NT = (((1,), (1,)), ((), ()))
TN = (((0,), (0,)), ((), ()))


def dot(a, b, dims=NN, precision=None):
    return lax.dot_general(a, b, dims, preferred_element_type=F32, precision=precision)


def rms(x, gain):
    return x * lax.rsqrt(jnp.mean(x * x, axis=-1, keepdims=True) + EPS) * gain


def loop(lo, hi, body):
    def step(j, carry):
        body(j)
        return carry

    lax.fori_loop(lo, hi, step, 0)


def kernel(
    n, nt,
    tok_in, gain, wq_in, wg_in, wv_in, wr_in, woa_in, wor_in, wk_in, wval_in, again, rgain, mapw, leak,
    extra_in, init_in,
    out_ref,
    tok, wq, wg, wv, wr, woa, wor, wk, wval, extra, init, out, in_sem, out_sem,
    gb, pk, nf, kvb, xb, xs, st, sd, un, ud, pb, db, sb, yr, zb, zr,
    col_send, col_recv, row_send, row_recv, tg_send, tg_recv, kg_send, kg_recv,
    k1_send, k1_recv, x_send, x_recv, un_send, un_recv, ud_send, ud_recv,
    d_send, d_recv, y_send, y_recv, z_send, z_recv,
):
    s, t = lax.axis_index("sp"), lax.axis_index("tp")
    count_p, count_z, count_h = n // 2, n // 4, nt // 2
    small = count_p <= 4
    x, p = s % 2, s // 2
    zl, zh = p % 2, p // 2
    hi, lo = t // 2, t % 2
    zmate, xmate, cmate = s + 2 - 4 * zl, s + 1 - 2 * x, t + 1 - 2 * lo

    def remote(src, dst, send_sem, recv_sem, device):
        return pltpu.make_async_remote_copy(
            src_ref=src, dst_ref=dst, send_sem=send_sem, recv_sem=recv_sem,
            device_id=device, device_id_type=MESH,
        )

    order_in = (
        (wg_in, wg), (tok_in, tok), (wk_in, wk), (wval_in, wval), (wv_in, wv), (wq_in, wq),
        (extra_in, extra), (wr_in, wr), (woa_in, woa), (wor_in, wor), (init_in, init),
    )
    loads = [pltpu.make_async_copy(a, b, in_sem.at[i]) for i, (a, b) in enumerate(order_in)]
    for load in loads:
        load.start()
    barrier = pltpu.get_barrier_semaphore()

    def greet(peer):
        pl.semaphore_signal(barrier, inc=1, device_id=peer, device_id_type=MESH)

    loop(1, count_p, lambda j: greet((2 * ((p + j) % count_p) + x, t)))
    greet((xmate, t))
    greet((s, cmate))
    for k in range(1, count_h):
        greet((s, (t + 2 * k) % nt))

    def need(*refs):
        for load, (_, b) in zip(loads, order_in):
            if any(b is r for r in refs):
                load.wait()

    rows, width = tok.shape
    part, half, w = wg.shape[0], wg.shape[0] // 2, RECURRENT_WIDTH
    at_v, at_q, at_r, at_a, at_o = part, 2 * part, 2 * part + half, 3 * part + half, 4 * part
    groups = ((0, at_v), (at_v, at_r), (at_r, at_a), (at_a, 5 * part))

    def split(ref, lo_row):
        mine = pl.ds(pl.multiple_of(zl * w, w), w)
        other = pl.ds(pl.multiple_of((1 - zl) * w, w), w)
        gb[s, lo_row : lo_row + part] = ref[:, mine]
        pk[lo_row : lo_row + part] = ref[:, other]

    def split_narrow(ref, lo_row):
        v = ref[...]
        a = v.shape[1] // 2
        first = jnp.concatenate([v[:half, :a], v[half:, :a]], axis=1)
        second = jnp.concatenate([v[:half, a:], v[half:, a:]], axis=1)
        gb[s, lo_row : lo_row + half] = jnp.where(zl == 0, first, second)
        pk[lo_row : lo_row + half] = jnp.where(zl == 0, second, first)

    def sent(ref, sem):
        remote(ref, ref, sem, sem, (xmate, t)).wait_send()

    class Gather:
        def __init__(self, ref, send, recv, planes, extent, first):
            self.ref, self.send, self.recv, self.planes = ref, send, recv, planes
            self.pieces = (slice(0, first), slice(first, extent))

        def slot(self, zz, owner):
            if self.planes == 1:
                return self.ref.at[owner % nt]
            return self.ref.at[zl if zz == 0 else 1 - zl, owner % nt]

        def sems(self, kind, i):
            past = (0, self.planes, self.planes + count_h - 1, self.planes + count_h + 1)[kind]
            return self.send.at[min(kind, 1)], self.recv.at[past + i]

        def copy(self, kind, i, owner, zz, device):
            block = self.slot(zz, owner)
            return remote(block, block, *self.sems(kind, i), device)

        def blocks(self, count):
            return self.ref.at[0:count] if self.planes == 1 else self.ref.at[0, 0:count]

        def core_out(self, zz, k):
            return self.copy(0, zz, t + nt - 2 * k, zz, (s, cmate))

        def y_out(self, k):
            return self.copy(1, k - 1, t, 0, (s, (t + 2 * k) % nt))

        def y_in(self, k):
            return self.copy(1, k - 1, t + nt - 2 * k, 0, (s, (t + nt - 2 * k) % nt))

        def piece(self, zz, owner, h):
            return self.slot(zz, owner).at[self.pieces[h]]

        def z_out(self, h):
            block = self.piece(0, t, h)
            return remote(block, block, *self.sems(2, h), (zmate, t))

        def z_in(self, h):
            block = self.piece(1, t, h)
            return remote(block, block, *self.sems(2, h), (zmate, t))

        def zy_out(self, h, k):
            block = self.piece(1, t, h)
            return remote(block, block, *self.sems(3, k - 1), (s, (t + 2 * k) % nt))

        def zy_in(self, k):
            return self.copy(3, k - 1, t + nt - 2 * k, 1, (s, (t + nt - 2 * k) % nt))

        def start(self):
            for k in range(1, count_h):
                self.y_out(k).start()
            self.core_out(0, 0).start()

        def start_z(self):
            for h in (0, 1):
                self.z_out(h).start()

        def relay_z(self, h):
            self.z_in(h).wait_recv()
            for k in range(1, count_h):
                self.zy_out(h, k).start()
            if h == 1:
                self.core_out(1, 0).start()

        def relay_y(self):
            for k in range(1, count_h):
                self.y_in(k).wait_recv()
                self.core_out(0, k).start()

        def relay_zy(self):
            for k in range(1, count_h):
                self.zy_in(k).wait_recv()
                self.core_out(1, k).start()

        def arrive(self, zz):
            both = self.blocks(count_h)
            remote(both, both, *self.sems(0, zz), (s, cmate)).wait_recv()

        def finish(self):
            if self.planes == 1:
                sent(self.blocks(count_h), self.send.at[0])
                sent(self.blocks(count_h - 1), self.send.at[1])
            else:
                sent(self.blocks(nt), self.send.at[0])
                sent(self.blocks(nt - 1), self.send.at[1])

    tokens = Gather(nf, tg_send, tg_recv, 2, rows, (rows // 2 + 15) // 16 * 16)
    keyvals = Gather(kvb, kg_send, kg_recv, 1, 0, 0)

    def cut(ref, g, many=False):
        rows_of = slice(groups[g][0], groups[g][1])
        return ref.at[:, rows_of] if many else ref.at[rows_of]

    def col_out(p2, g, same):
        return remote(
            cut(gb.at[s], g) if same else cut(pk, g), cut(gb.at[s], g),
            col_send.at[0], col_recv.at[p, g], (2 * p2 + x, t),
        )

    def col_in(p2, g):
        slot = cut(gb.at[2 * p2 + x], g)
        return remote(slot, slot, col_send.at[0], col_recv.at[p2, g], (2 * p2 + x, t))

    def row_out(p2, g):
        slot = cut(gb.at[2 * p2 + x], g)
        return remote(slot, slot, row_send.at[0], row_recv.at[g if g < 2 else 2 + (g - 2) * count_p + p2], (xmate, t))

    def row_in(p2, g):
        slot = cut(gb.at[2 * p2 + 1 - x], g)
        return remote(slot, slot, row_send.at[0], row_recv.at[g if g < 2 else 2 + (g - 2) * count_p + p2], (xmate, t))

    def near(d, body, skip=-1):
        for sign in (1, -1):
            p2 = p + sign * d

            @pl.when((p2 >= 0) & (p2 < count_p) & (p2 != skip))
            def _():
                body(p2)

    def distances(body):
        if small:
            for d in range(1, count_p):
                body(d, d % 2 == 0)
        else:
            loop(0, count_p // 2, lambda i: body(2 * i + 1, False))
            loop(1, count_p // 2, lambda i: body(2 * i, True))

    at_edge = (p == 0) | (p == count_p - 1)

    def at_end(body):
        if small:
            pl.when(at_edge)(body)

    def at_middle(body):
        if small:
            pl.when(jnp.logical_not(at_edge))(body)
        else:
            body()

    def to_mate(g):
        if small:
            col_out(p + 1 - 2 * zl, g, False).start()

    def to_rest(g):
        if small:
            for d in range(1, count_p):
                near(d, lambda p2: col_out(p2, g, d % 2 == 0).start(), p + 1 - 2 * zl)
        else:
            distances(lambda d, same: near(d, lambda p2: col_out(p2, g, same).start()))

    def columns(g):
        to_mate(g)
        to_rest(g)

    sources = (count_z - zh, p + 1 - 2 * zl, (count_p - 1) * (1 - zh))

    def forward_one(g, p2):
        col_in(p2, g).wait_recv()
        row_out(p2, g).start()

    def forward(g, i):
        if small:
            forward_one(g, sources[i])
        elif i == 0:
            loop(1, count_p, lambda e: near(e, lambda p2: forward_one(g, p2)))

    def collect(g):
        if g < 2:
            column = cut(gb.at[0:count_p], g, True)
            remote(column, column, row_send.at[0], row_recv.at[g], (xmate, t)).wait_recv()
        else:
            loop(0, count_p, lambda p2: row_in(p2, g).wait_recv())

    def k1_copy(j, owner):
        block = kvb.at[t, x, owner % count_p]
        peer = (p + j) % count_p
        return remote(block, block, k1_send.at[0], k1_recv.at[0], (2 * peer + x, t))

    def swap(i, src, dst, device):
        return remote(src, dst, x_send.at[i], x_recv.at[i], device)

    def kv_swap(side):
        return swap(0, kvb.at[t, side], kvb.at[t, side], (xmate, t))

    def extra_swap():
        return swap(1, xs, xb, (zmate, t))

    def st_swap(side):
        return swap(2, st.at[side], st.at[side], (xmate, t))

    def sd_swap(side):
        return swap(3, sd.at[side], sd.at[side], (xmate, t))

    need(wg)
    split(wg, 0)
    pl.semaphore_wait(barrier, count_p + count_h)
    row_out(p, 0).start()
    to_mate(0)
    at_middle(lambda: to_rest(0))
    need(tok)
    normed = rms(tok[...].astype(F32), gain[...]).astype(BF16)
    nf[zl, t] = normed
    need(wk, wval)
    kvb[t, x, p] = jnp.concatenate(
        [dot(normed, wk[...], NT).astype(BF16), dot(normed, wval[...], NT).astype(BF16)], axis=1
    )
    loop(1, count_p, lambda j: k1_copy(j, p).start())
    tokens.start()
    need(wv, wq)
    split(wv, at_v)
    split_narrow(wq, at_q)
    row_out(p, 1).start()
    to_mate(1)
    at_middle(lambda: to_rest(1))
    tokens.start_z()

    def far():
        to_rest(0)
        to_rest(1)

    at_end(far)
    need(extra)
    xs[...] = extra[:, pl.ds(pl.multiple_of((1 - zl) * w, w), w)].astype(BF16)
    extra_swap().start()
    need(wr, woa, wor, init)
    split(wr, at_r)
    split_narrow(woa, at_a)
    split(wor, at_o)
    forward(0, 1)
    forward(0, 0)
    others = kvb.at[0, 0, 0 : count_p - 1]
    remote(others, others, k1_send.at[0], k1_recv.at[0], (xmate, t)).wait_recv()
    kv_swap(x).start()
    row_out(p, 2).start()
    tokens.relay_y()
    forward(1, 1)
    forward(1, 0)
    row_out(p, 3).start()
    kv_swap(1 - x).wait_recv()
    keyvals.start()
    columns(2)
    tokens.relay_z(0)
    forward(0, 2)
    tokens.relay_z(1)
    forward(1, 2)
    columns(3)
    keyvals.relay_y()
    tokens.relay_zy()
    at_middle(lambda: forward(2, 0))
    at_middle(lambda: forward(2, 1))
    at_end(lambda: forward(2, 1))

    def on_core(c, body):
        pl.when(lo == c)(body)

    def last_two():
        forward(2, 2)
        forward(2, 0)

    at_end(lambda: on_core(1, last_two))
    tokens.arrive(0)
    tokens.arrive(1)
    extra_swap().wait_recv()
    collect(0)

    block = nt * rows
    full = nf[...].reshape(2 * block, width)

    def weight(lo_row):
        return gb[:, lo_row : lo_row + part].reshape(n * part, w)

    def widen(v):
        a = v.shape[2] // 2
        both = jnp.concatenate([v[:, :, :a], v[:, :, a:]], axis=1)
        return both.reshape(both.shape[0] * both.shape[1], a)

    gate = dot(full, weight(0)).astype(BF16).astype(F32)
    leak_mine = jnp.where(zl == 0, leak[:, :w], leak[:, w:])
    inflow = leak_mine * (1.0 - jax.nn.sigmoid(gate))
    here = extra[:, pl.ds(pl.multiple_of(zl * w, w), w)]
    there = xb[...].astype(F32)
    added = jnp.concatenate([jnp.where(zl == 0, here, there), jnp.where(zl == 0, there, here)], axis=0)
    log_decay = jnp.log(1.0 - inflow) + added
    spans = block // REC_SPAN
    rr = lax.broadcasted_iota(jnp.int32, (REC_SPAN, REC_SPAN), 0)
    cc = lax.broadcasted_iota(jnp.int32, (REC_SPAN, REC_SPAN), 1)
    lower = (rr >= cc).astype(F32)
    running, offsets, befores, weighted, grown, shrunk = [], [], [], [], [], []
    for j in (0, 1):
        offset = jnp.zeros((1, w), F32)
        for i in range(spans):
            r = slice(j * block + i * REC_SPAN, j * block + (i + 1) * REC_SPAN)
            run = dot(lower, log_decay[r], precision=lax.Precision.HIGHEST)
            final = run[REC_SPAN - 1 : REC_SPAN]
            running.append(run)
            offsets.append(offset)
            offset = offset + final
            weighted.append((inflow[r] * jnp.exp(final - run)).astype(BF16))
            grown.append(jnp.exp(run))
            shrunk.append((inflow[r] * jnp.exp(-run)).astype(BF16))
        sd[x, j] = jnp.broadcast_to(offset, sd.shape[2:])
    at_middle(lambda: forward(2, 2))
    at_end(lambda: on_core(0, last_two))
    collect(1)
    both = dot(full, jnp.concatenate([weight(at_v), widen(gb[:, at_q:at_r])], axis=1)).astype(BF16)
    vals, queries = both[:, :w], both[:, w:]
    for j in (0, 1):
        carried = None
        for i in range(spans):
            r = slice(j * block + i * REC_SPAN, j * block + (i + 1) * REC_SPAN)
            final = running[j * spans + i][REC_SPAN - 1 : REC_SPAN]
            befores.append(carried)
            new = dot(vals[r], weighted[j * spans + i], TN)
            carried = new if carried is None else carried * jnp.exp(final) + new
        st[x, j] = carried.astype(BF16)
    st_swap(x).start()
    sd_swap(x).start()


    def advance(carried, sx, j):
        return carried * jnp.exp(sd[sx, j][0:1]) + st[sx, j].astype(F32)

    def un_pair(z2, owner):
        device = (4 * z2 + 2 * zl + x, t)
        return (
            remote(un.at[owner], un.at[owner], un_send.at[z2], un_recv.at[owner], device),
            remote(ud.at[owner], ud.at[owner], ud_send.at[z2], ud_recv.at[owner], device),
        )

    def un_start(z2):
        for copy in un_pair(z2, zh):
            copy.start()

    def un_wait(owner):
        for copy in un_pair(owner, owner):
            copy.wait_recv()

    def join_units():
        st_swap(1 - x).wait_recv()
        sd_swap(1 - x).wait_recv()
        unit = st[0, 0].astype(F32)
        for sx, j in ((1, 0), (0, 1), (1, 1)):
            unit = advance(unit, sx, j)
        un[zh] = unit.astype(BF16)
        ud[zh] = sd[0, 0] + sd[1, 0] + sd[0, 1] + sd[1, 1]
        loop(zh + 1, count_z, un_start)

    def un_done(z2):
        for copy in un_pair(z2, zh):
            copy.wait_send()

    keyvals.arrive(0)

    forward(3, 1)
    zs = max(1, min(count_p, KEY_BLOCK // (2 * block)))
    blocks = count_p // zs
    scale = math.log2(math.e) / math.sqrt(QK_DIM)

    def attend(query, b):
        both = kvb[:, :, pl.ds(b * zs, zs)].reshape(2 * zs * block, kvb.shape[4])
        values = both[:, 2 * QK_DIM :]
        parts = []
        for comp in range(2):
            cols = slice(comp * QK_DIM, (comp + 1) * QK_DIM)
            scores = dot(query[:, cols], both[:, cols], NT)
            peak = jnp.max(scores, axis=1, keepdims=True)
            expo = jnp.exp2((scores - peak) * scale)
            parts += [peak, jnp.sum(expo, axis=1, keepdims=True), dot(expo.astype(BF16), values)]
        return tuple(parts)

    def merge(a, b):
        parts = []
        for comp in range(2):
            pa, ta, wa = a[3 * comp : 3 * comp + 3]
            pc, tc, wc = b[3 * comp : 3 * comp + 3]
            peak = jnp.maximum(pa, pc)
            ea, ec = jnp.exp2((pa - peak) * scale), jnp.exp2((pc - peak) * scale)
            parts += [peak, ta * ea + tc * ec, wa * ea + wc * ec]
        return tuple(parts)

    hidden = []
    for j in (0, 1):
        query = queries[j * block : (j + 1) * block]
        got = attend(query, 0)
        if blocks > 1:
            got = lax.fori_loop(1, blocks, lambda b, g: merge(g, attend(query, b)), got)
        blended = got[2] / got[1] - mapw[zl] * (got[5] / got[4])
        hidden.append(rms(blended, again[...]))
    attn_hidden = jnp.concatenate(hidden, axis=0).astype(BF16)

    def raw_term(owner):
        rows_in = nf[:, :, :, pl.ds(pl.multiple_of(owner * part, part), part)]
        return dot(rows_in.reshape(2 * block, part), gb[owner, at_r:at_a])

    stepwise = small and part % 128 == 0
    pieces = (p, sources[1], sources[2], sources[0])
    if stepwise:
        raw = raw_term(2 * pieces[0] + x)
        for q in pieces[1:]:
            raw = raw + raw_term(2 * q + x)
    join_units()
    forward(3, 2)
    if stepwise:
        for q in pieces:
            row_in(q, 2).wait_recv()
            raw = raw + raw_term(2 * q + 1 - x)
    else:
        collect(2)
        raw = dot(full, weight(at_r))
    raw = raw.astype(BF16).astype(F32)
    rec_query = raw * jax.nn.sigmoid(raw)
    local, lifted = [], []
    for j in (0, 1):
        outs, lifts = [], []
        for i in range(spans):
            r = slice(j * block + i * REC_SPAN, j * block + (i + 1) * REC_SPAN)
            m = j * spans + i
            decayed = rec_query[r] * grown[m]
            dq = decayed.astype(BF16)
            within = dot(dq, shrunk[m], NT) * lower
            o = dot(within.astype(BF16), vals[r])
            if befores[m] is not None:
                o = o + dot(dq, befores[m].astype(BF16), NT)
            outs.append(o)
            lifts.append(decayed * jnp.exp(offsets[m]))
        local.append(jnp.concatenate(outs, axis=0))
        lifted.append(jnp.concatenate(lifts, axis=0).astype(BF16))

    forward(3, 0)
    loop(0, zh, un_wait)

    def chain(k, carry):
        return carry * jnp.exp(ud[k][0:1]) + un[k].astype(F32)

    base = lax.fori_loop(0, zh, chain, init[zl].T)
    s01 = advance(base, 0, 0)
    s10 = advance(s01, 1, 0)
    s11 = advance(s10, 0, 1)
    incoming = (jnp.where(x == 0, base, s01), jnp.where(x == 0, s10, s11))
    rec = []
    for j in (0, 1):
        o = local[j] + dot(lifted[j], incoming[j].astype(BF16), NT)
        rec.append(rms(o, rgain[...]))
    rec_hidden = jnp.concatenate(rec, axis=0).astype(BF16)
    both_hidden = jnp.concatenate([rec_hidden, attn_hidden], axis=1)

    per = pb.shape[5] // part
    fw = per * part
    chunks = n // per

    def d_copy(ch):
        return remote(pb.at[ch, 1 - lo], db.at[ch], d_send.at[0], d_recv.at[ch], (s, cmate))

    def y_copy(ch, k, flip):
        h2 = (hi + k) % count_h
        src = zb.at[ch, pl.ds(h2, 1)] if flip else sb.at[ch, pl.ds(2 * h2, 2)]
        dst = yr.at[ch, k, pl.ds(0, 1)] if flip else yr.at[ch, k]
        return remote(src, dst, y_send.at[int(flip)], y_recv.at[ch, k - 1], (s, 2 * h2 + lo))

    def z_copy(ch, flip):
        src = sb.at[ch, pl.ds(count_h * (1 - zl), count_h)] if flip else zb.at[ch, pl.ds(1 - zl, 1)]
        dst = zr.at[ch] if flip else zr.at[ch, pl.ds(0, 1)]
        return remote(src, dst, z_send.at[int(flip)], z_recv.at[ch], (zmate, t))

    def stage_d(ch):
        shard = gb[pl.ds(ch * per, per)]
        weights = jnp.concatenate(
            [shard[:, at_o:].reshape(fw, w), widen(shard[:, at_a:at_o])], axis=1
        )
        got = dot(both_hidden, weights, NT).astype(BF16)
        for z2 in (0, 1):
            for t2 in range(nt):
                lo_row = (z2 * nt + t2) * rows
                pb[ch, t2 % 2, z2, t2 // 2] = got[lo_row : lo_row + rows]
        d_copy(ch).start()

    def stage_first(ch, flip):
        d_copy(ch).wait_recv()
        total = (pb[ch, lo].astype(F32) + db[ch].astype(F32)).astype(BF16)
        if flip:
            sb[ch] = total.reshape(sb.shape[1:])
            z_copy(ch, flip).start()
        else:
            for h2 in range(count_h):
                sb[ch, 2 * h2 : 2 * h2 + 2] = total[:, h2]
            for k in range(1, count_h):
                y_copy(ch, k, flip).start()

    def stage_second(ch, flip):
        if flip:
            z_copy(ch, flip).wait_recv()
            mine = sb[ch, pl.ds(count_h * zl, count_h)]
            zb[ch] = (mine.astype(F32) + zr[ch].astype(F32)).astype(BF16)
            for k in range(1, count_h):
                y_copy(ch, k, flip).start()
        else:
            total = sb[ch, pl.ds(2 * hi, 2)].astype(F32)
            for k in range(1, count_h):
                y_copy(ch, k, flip).wait_recv()
                total = total + yr[ch, k].astype(F32)
            zb[ch, 0:2] = total.astype(BF16)
            z_copy(ch, flip).start()

    def stage_out(ch, flip):
        if flip:
            total = zb[ch, hi].astype(F32)
            for k in range(1, count_h):
                y_copy(ch, k, flip).wait_recv()
                total = total + yr[ch, k, 0].astype(F32)
        else:
            z_copy(ch, flip).wait_recv()
            total = zb[ch, zl].astype(F32) + zr[ch, 0].astype(F32)
        out[:, pl.ds(pl.multiple_of(ch * fw, fw), fw)] = total.astype(out.dtype)
        store(ch).start()

    def store(ch):
        cols = pl.ds(pl.multiple_of(ch * fw, fw), fw)
        return pltpu.make_async_copy(out.at[:, cols], out_ref.at[:, cols], out_sem.at[0])

    if small and per == 1:
        order = [(q, c) for c in (0, 1) for q in (2 * zh, 2 * zh + 1)]
        order += [(q, c) for q in (sources[2], sources[0]) for c in (0, 1)]
        ready = []
        for q, c in order:
            ready.append((2 * q + x if c == 0 else 2 * q + 1 - x, q if c == 1 else None))
    else:
        collect(3)
        ready = [(ch, None) for ch in range(chunks)]

    lag = len(ready)
    for i in range(lag + LAGS[2]):
        if i < lag:
            ch, q = ready[i]
            if q is not None:
                row_in(q, 3).wait_recv()
            stage_d(ch)
        for body, late in zip((stage_first, stage_second, stage_out), LAGS):
            if 0 <= i - late < lag:
                body(ready[i - late][0], (i - late) % 2 == 1)

    sent(gb.at[0 : count_p - 1], col_send.at[0])
    sent(gb.at[0:count_p], row_send.at[0])
    tokens.finish()
    keyvals.finish()
    sent(others, k1_send.at[0])
    kv_swap(x).wait_send()
    extra_swap().wait_send()
    st_swap(x).wait_send()
    sd_swap(x).wait_send()
    loop(zh + 1, count_z, un_done)

    odd = chunks // 2
    even = chunks - odd
    sent(yr.at[0:even, 0 : count_h - 1], y_send.at[0])
    sent(zb.at[0:even, 0:1], z_send.at[0])
    sent(zb.at[0:odd, 0 : count_h - 1], y_send.at[1])
    sent(zb.at[0:odd, 0:count_h], z_send.at[1])
    sent(db, d_send.at[0])
    pltpu.make_async_copy(out, out_ref, out_sem.at[0]).wait()


def solution(mesh):
    n, nt = mesh.shape["sp"], mesh.shape["tp"]

    def body(
        tokens, input_norm_gain, paired_query_weight, shared_key_weight, shared_value_weight,
        recurrent_query_weight, forget_gate_weight, recurrent_value_weight,
        attention_output_weight, recurrent_output_weight, attention_head_gain,
        recurrent_head_gain, second_map_weight, forget_leak_rate, extra_log_decay,
        initial_recurrent_state,
    ):
        rows, width = tokens.shape
        weights = (
            paired_query_weight, forget_gate_weight, recurrent_value_weight,
            recurrent_query_weight, attention_output_weight, recurrent_output_weight,
        )
        part = forget_gate_weight.shape[0]
        span = extra_log_decay.shape[0]
        count_p, count_z, count_h = n // 2, n // 4, nt // 2
        fw = part * max(1, OUT_WIDTH // part)
        chunks = width // fw
        kv_width = 2 * QK_DIM + HEAD_DIM
        wk, wval = shared_key_weight.T, shared_value_weight.T
        staged = (tokens, *weights, wk, wval, extra_log_decay, initial_recurrent_state)
        hb = pl.BlockSpec(memory_space=pl.ANY)
        vm = pl.BlockSpec(memory_space=pltpu.VMEM)
        sm = pl.BlockSpec(memory_space=pltpu.SMEM)
        dma = pltpu.SemaphoreType.DMA
        w = RECURRENT_WIDTH
        return pl.pallas_call(
            functools.partial(kernel, n, nt),
            out_shape=jax.ShapeDtypeStruct((rows, width), BF16),
            in_specs=[hb, vm] + [hb] * 8 + [vm] * 2 + [sm, vm, hb, hb],
            out_specs=hb,
            scratch_shapes=[pltpu.VMEM(a.shape, a.dtype) for a in staged] + [
                pltpu.VMEM((rows, width), BF16),
                dma((len(staged),)), dma((1,)),
                pltpu.VMEM((n, 5 * part, w), BF16),
                pltpu.VMEM((5 * part, w), BF16),
                pltpu.VMEM((2, nt, rows, width), BF16),
                pltpu.VMEM((nt, 2, count_p, rows, kv_width), BF16),
                pltpu.VMEM((span, w), BF16),
                pltpu.VMEM((span, w), BF16),
                pltpu.VMEM((2, 2, w, w), BF16),
                pltpu.VMEM((2, 2, 8, w), F32),
                pltpu.VMEM((count_z, w, w), BF16),
                pltpu.VMEM((count_z, 8, w), F32),
                pltpu.VMEM((chunks, 2, 2, count_h, rows, fw), BF16),
                pltpu.VMEM((chunks, 2, count_h, rows, fw), BF16),
                pltpu.VMEM((chunks, 2 * count_h, rows, fw), BF16),
                pltpu.VMEM((chunks, count_h, 2, rows, fw), BF16),
                pltpu.VMEM((chunks, max(2, count_h), rows, fw), BF16),
                pltpu.VMEM((chunks, max(2, count_h), rows, fw), BF16),
                dma((1,)), dma((count_p, 4)),
                dma((1,)), dma((2 + 2 * count_p,)),
                dma((2,)), dma((2 * count_h + 2,)),
                dma((2,)), dma((count_h,)),
                dma((1,)), dma((1,)),
                dma((4,)), dma((4,)),
                dma((count_z,)), dma((count_z,)),
                dma((count_z,)), dma((count_z,)),
                dma((1,)), dma((chunks,)),
                dma((2,)), dma((chunks, count_h - 1)),
                dma((2,)), dma((chunks,)),
            ],
            compiler_params=pltpu.CompilerParams(
                has_side_effects=True, collective_id=0, vmem_limit_bytes=60 * 1024 * 1024
            ),
        )(
            tokens, input_norm_gain[None], *weights, wk, wval,
            attention_head_gain[None], recurrent_head_gain[None], second_map_weight,
            forget_leak_rate[None], extra_log_decay, initial_recurrent_state,
        )

    placed = (
        P(("sp", "tp"), None), P(), P("sp", "tp"), P(), P(), P("sp", "tp"), P("sp", "tp"),
        P("sp", "tp"), P("sp", "tp"), P("sp", "tp"), P(), P(), P("tp"), P("tp"),
        P("sp", "tp"), P("tp", None, None),
    )
    return jax.shard_map(
        body, mesh=mesh, in_specs=placed, out_specs=P(("sp", "tp"), None), check_vma=False
    )
```

```python
import functools
import math

import jax
import jax.numpy as jnp
from jax import lax
from jax.experimental import pallas as pl
from jax.experimental.pallas import tpu as pltpu
from jax.sharding import PartitionSpec as P

QK_DIM = 32
HEAD_DIM = 64
RECURRENT_WIDTH = 128
REC_SPAN = 64
KEY_BLOCK = 1536
OUT_WIDTH = 256
LAGS = (2, 9, 15)
EPS = 1e-06
MESH = pl.DeviceIdType.MESH
F32, BF16 = jnp.float32, jnp.bfloat16

NN = (((1,), (0,)), ((), ()))
NT = (((1,), (1,)), ((), ()))
TN = (((0,), (0,)), ((), ()))


def dot(a, b, dims=NN, precision=None):
    return lax.dot_general(a, b, dims, preferred_element_type=F32, precision=precision)


def rms(x, gain):
    return x * lax.rsqrt(jnp.mean(x * x, axis=-1, keepdims=True) + EPS) * gain


def loop(lo, hi, body):
    def step(j, carry):
        body(j)
        return carry

    lax.fori_loop(lo, hi, step, 0)


def kernel(
    n, nt,
    tok_in, gain_in, wq_in, wg_in, wv_in, wr_in, woa_in, wor_in, wk_in, wval_in, again_in, rgain_in,
    mapw_in, leak_in, extra_in, init_in,
    out_ref,
    tok, gain, wq, wg, wv, wr, woa, wor, wk, wval, again, rgain, mapw, leak, extra, init, out,
    in_sem, out_sem,
    gb, pk, nf, kvb, xb, xs, st, sd, un, ud, pb, db, sb, yr, zb, zr,
    col_send, col_recv, row_send, row_recv, tg_send, tg_recv, kg_send, kg_recv,
    k1_send, k1_recv, x_send, x_recv, un_send, un_recv, ud_send, ud_recv,
    d_send, d_recv, y_send, y_recv, z_send, z_recv,
):
    s, t = lax.axis_index("sp"), lax.axis_index("tp")
    count_p, count_z, count_h = n // 2, n // 4, nt // 2
    small = count_p <= 4
    x, p = s % 2, s // 2
    zl, zh = p % 2, p // 2
    hi, lo = t // 2, t % 2
    zmate, xmate, cmate = s + 2 - 4 * zl, s + 1 - 2 * x, t + 1 - 2 * lo

    def remote(src, dst, send_sem, recv_sem, device):
        return pltpu.make_async_remote_copy(
            src_ref=src, dst_ref=dst, send_sem=send_sem, recv_sem=recv_sem,
            device_id=device, device_id_type=MESH,
        )

    barrier = pltpu.get_barrier_semaphore()

    def greet(peer):
        pl.semaphore_signal(barrier, inc=1, device_id=peer, device_id_type=MESH)

    loop(1, count_p, lambda j: greet((2 * ((p + j) % count_p) + x, t)))
    greet((xmate, t))
    greet((s, cmate))
    for k in range(1, count_h):
        greet((s, (t + 2 * k) % nt))

    order_in = (
        (wg_in, wg), (tok_in, tok), (gain_in, gain), (wk_in, wk), (wval_in, wval), (wv_in, wv),
        (wq_in, wq), (extra_in, extra), (wr_in, wr), (woa_in, woa), (wor_in, wor), (init_in, init),
        (again_in, again), (rgain_in, rgain), (mapw_in, mapw), (leak_in, leak),
    )
    loads = [pltpu.make_async_copy(a, b, in_sem.at[i]) for i, (a, b) in enumerate(order_in)]
    for load in loads:
        load.start()

    def need(*refs):
        for load, (_, b) in zip(loads, order_in):
            if any(b is r for r in refs):
                load.wait()

    rows, width = tok.shape
    part, half, w = wg.shape[0], wg.shape[0] // 2, RECURRENT_WIDTH
    at_v, at_q, at_r, at_a, at_o = part, 2 * part, 2 * part + half, 3 * part + half, 4 * part
    groups = ((0, at_v), (at_v, at_r), (at_r, at_a), (at_a, 5 * part))

    def split(ref, lo_row):
        mine = pl.ds(pl.multiple_of(zl * w, w), w)
        other = pl.ds(pl.multiple_of((1 - zl) * w, w), w)
        gb[s, lo_row : lo_row + part] = ref[:, mine]
        pk[lo_row : lo_row + part] = ref[:, other]

    def split_narrow(ref, lo_row):
        v = ref[...]
        a = v.shape[1] // 2
        first = jnp.concatenate([v[:half, :a], v[half:, :a]], axis=1)
        second = jnp.concatenate([v[:half, a:], v[half:, a:]], axis=1)
        gb[s, lo_row : lo_row + half] = jnp.where(zl == 0, first, second)
        pk[lo_row : lo_row + half] = jnp.where(zl == 0, second, first)

    def sent(ref, sem):
        remote(ref, ref, sem, sem, (xmate, t)).wait_send()

    class Gather:
        def __init__(self, ref, send, recv, planes, extent, first):
            self.ref, self.send, self.recv, self.planes = ref, send, recv, planes
            self.pieces = (slice(0, first), slice(first, extent))

        def slot(self, zz, owner):
            if self.planes == 1:
                return self.ref.at[owner % nt]
            return self.ref.at[zl if zz == 0 else 1 - zl, owner % nt]

        def sems(self, kind, i):
            past = (0, self.planes, self.planes + count_h - 1, self.planes + count_h + 1)[kind]
            return self.send.at[min(kind, 1)], self.recv.at[past + i]

        def copy(self, kind, i, owner, zz, device):
            block = self.slot(zz, owner)
            return remote(block, block, *self.sems(kind, i), device)

        def blocks(self, count):
            return self.ref.at[0:count] if self.planes == 1 else self.ref.at[0, 0:count]

        def core_out(self, zz, k):
            return self.copy(0, zz, t + nt - 2 * k, zz, (s, cmate))

        def y_out(self, k):
            return self.copy(1, k - 1, t, 0, (s, (t + 2 * k) % nt))

        def y_in(self, k):
            return self.copy(1, k - 1, t + nt - 2 * k, 0, (s, (t + nt - 2 * k) % nt))

        def piece(self, zz, owner, h):
            return self.slot(zz, owner).at[self.pieces[h]]

        def z_out(self, h):
            block = self.piece(0, t, h)
            return remote(block, block, *self.sems(2, h), (zmate, t))

        def z_in(self, h):
            block = self.piece(1, t, h)
            return remote(block, block, *self.sems(2, h), (zmate, t))

        def zy_out(self, h, k):
            block = self.piece(1, t, h)
            return remote(block, block, *self.sems(3, k - 1), (s, (t + 2 * k) % nt))

        def zy_in(self, k):
            return self.copy(3, k - 1, t + nt - 2 * k, 1, (s, (t + nt - 2 * k) % nt))

        def start(self):
            for k in range(1, count_h):
                self.y_out(k).start()
            self.core_out(0, 0).start()

        def start_z(self):
            for h in (0, 1):
                self.z_out(h).start()

        def relay_z(self, h):
            self.z_in(h).wait_recv()
            for k in range(1, count_h):
                self.zy_out(h, k).start()
            if h == 1:
                self.core_out(1, 0).start()

        def relay_y(self):
            for k in range(1, count_h):
                self.y_in(k).wait_recv()
                self.core_out(0, k).start()

        def relay_zy(self):
            for k in range(1, count_h):
                self.zy_in(k).wait_recv()
                self.core_out(1, k).start()

        def arrive(self, zz):
            both = self.blocks(count_h)
            remote(both, both, *self.sems(0, zz), (s, cmate)).wait_recv()

        def finish(self):
            if self.planes == 1:
                sent(self.blocks(count_h), self.send.at[0])
                sent(self.blocks(count_h - 1), self.send.at[1])
            else:
                sent(self.blocks(nt), self.send.at[0])
                sent(self.blocks(nt - 1), self.send.at[1])

    tokens = Gather(nf, tg_send, tg_recv, 2, rows, (rows // 2 + 15) // 16 * 16)
    keyvals = Gather(kvb, kg_send, kg_recv, 1, 0, 0)

    def cut(ref, g, many=False):
        rows_of = slice(groups[g][0], groups[g][1])
        return ref.at[:, rows_of] if many else ref.at[rows_of]

    def col_out(p2, g, same):
        return remote(
            cut(gb.at[s], g) if same else cut(pk, g), cut(gb.at[s], g),
            col_send.at[0], col_recv.at[p, g], (2 * p2 + x, t),
        )

    def col_in(p2, g):
        slot = cut(gb.at[2 * p2 + x], g)
        return remote(slot, slot, col_send.at[0], col_recv.at[p2, g], (2 * p2 + x, t))

    def row_out(p2, g):
        slot = cut(gb.at[2 * p2 + x], g)
        return remote(slot, slot, row_send.at[0], row_recv.at[g if g < 2 else 2 + (g - 2) * count_p + p2], (xmate, t))

    def row_in(p2, g):
        slot = cut(gb.at[2 * p2 + 1 - x], g)
        return remote(slot, slot, row_send.at[0], row_recv.at[g if g < 2 else 2 + (g - 2) * count_p + p2], (xmate, t))

    def near(d, body, skip=-1):
        for sign in (1, -1):
            p2 = p + sign * d

            @pl.when((p2 >= 0) & (p2 < count_p) & (p2 != skip))
            def _():
                body(p2)

    def distances(body):
        if small:
            for d in range(1, count_p):
                body(d, d % 2 == 0)
        else:
            loop(0, count_p // 2, lambda i: body(2 * i + 1, False))
            loop(1, count_p // 2, lambda i: body(2 * i, True))

    def on_core(c, body):
        pl.when(lo == c)(body)

    at_edge = (p == 0) | (p == count_p - 1)

    def at_end(body):
        if small:
            pl.when(at_edge)(body)

    def at_middle(body):
        if small:
            pl.when(jnp.logical_not(at_edge))(body)
        else:
            body()

    def to_mate(g):
        if small:
            col_out(p + 1 - 2 * zl, g, False).start()

    def to_rest(g):
        if small:
            for d in range(1, count_p):
                near(d, lambda p2: col_out(p2, g, d % 2 == 0).start(), p + 1 - 2 * zl)
        else:
            distances(lambda d, same: near(d, lambda p2: col_out(p2, g, same).start()))

    def columns(g):
        to_mate(g)
        to_rest(g)

    sources = (count_z - zh, p + 1 - 2 * zl, (count_p - 1) * (1 - zh))

    def forward_one(g, p2):
        col_in(p2, g).wait_recv()
        row_out(p2, g).start()

    def forward(g, i):
        if small:
            forward_one(g, sources[i])
        elif i == 0:
            loop(1, count_p, lambda e: near(e, lambda p2: forward_one(g, p2)))

    def collect(g):
        if g < 2:
            column = cut(gb.at[0:count_p], g, True)
            remote(column, column, row_send.at[0], row_recv.at[g], (xmate, t)).wait_recv()
        else:
            loop(0, count_p, lambda p2: row_in(p2, g).wait_recv())

    def k1_copy(j, owner):
        block = kvb.at[t, x, owner % count_p]
        peer = (p + j) % count_p
        return remote(block, block, k1_send.at[0], k1_recv.at[0], (2 * peer + x, t))

    def swap(i, src, dst, device):
        return remote(src, dst, x_send.at[i], x_recv.at[i], device)

    def kv_swap(side):
        return swap(0, kvb.at[t, side], kvb.at[t, side], (xmate, t))

    def extra_swap():
        return swap(1, xs, xb, (zmate, t))

    def st_swap(side):
        return swap(2, st.at[side], st.at[side], (xmate, t))

    def sd_swap(side):
        return swap(3, sd.at[side], sd.at[side], (xmate, t))

    need(wg)
    split(wg, 0)
    pl.semaphore_wait(barrier, count_p + count_h)
    row_out(p, 0).start()
    to_mate(0)
    at_middle(lambda: to_rest(0))
    need(tok, gain)
    normed = rms(tok[...].astype(F32), gain[...]).astype(BF16)
    nf[zl, t] = normed
    need(wk, wval)
    kvb[t, x, p] = jnp.concatenate(
        [dot(normed, wk[...], NT).astype(BF16), dot(normed, wval[...], NT).astype(BF16)], axis=1
    )
    loop(1, count_p, lambda j: k1_copy(j, p).start())
    tokens.start()
    need(wv, wq)
    split(wv, at_v)
    split_narrow(wq, at_q)
    row_out(p, 1).start()
    to_mate(1)
    at_middle(lambda: to_rest(1))
    tokens.start_z()

    def far():
        to_rest(0)
        to_rest(1)

    at_end(far)
    need(extra)
    xs[...] = extra[:, pl.ds(pl.multiple_of((1 - zl) * w, w), w)].astype(BF16)
    extra_swap().start()
    need(wr, woa, wor, init, again, rgain, mapw, leak)
    split(wr, at_r)
    split_narrow(woa, at_a)
    split(wor, at_o)
    forward(0, 1)
    forward(0, 0)
    others = kvb.at[0, 0, 0 : count_p - 1]
    remote(others, others, k1_send.at[0], k1_recv.at[0], (xmate, t)).wait_recv()
    kv_swap(x).start()
    row_out(p, 2).start()
    tokens.relay_y()
    forward(1, 1)
    forward(1, 0)
    row_out(p, 3).start()
    kv_swap(1 - x).wait_recv()
    keyvals.start()
    columns(2)
    tokens.relay_z(0)
    forward(0, 2)
    tokens.relay_z(1)
    forward(1, 2)
    columns(3)
    keyvals.relay_y()
    tokens.relay_zy()
    at_middle(lambda: forward(2, 0))
    at_middle(lambda: forward(2, 1))
    at_end(lambda: on_core(1, lambda: forward(2, 1)))

    def last_two():
        forward(2, 2)
        forward(2, 0)

    at_end(lambda: on_core(1, last_two))
    tokens.arrive(0)
    tokens.arrive(1)
    extra_swap().wait_recv()
    collect(0)

    block = nt * rows
    full = nf[...].reshape(2 * block, width)

    def weight(lo_row):
        return gb[:, lo_row : lo_row + part].reshape(n * part, w)

    def widen(v):
        a = v.shape[2] // 2
        both = jnp.concatenate([v[:, :, :a], v[:, :, a:]], axis=1)
        return both.reshape(both.shape[0] * both.shape[1], a)

    gate = dot(full, weight(0)).astype(BF16).astype(F32)
    leak_mine = jnp.where(zl == 0, leak[:, :w], leak[:, w:])
    inflow = leak_mine * (1.0 - jax.nn.sigmoid(gate))
    here = extra[:, pl.ds(pl.multiple_of(zl * w, w), w)]
    there = xb[...].astype(F32)
    added = jnp.concatenate([jnp.where(zl == 0, here, there), jnp.where(zl == 0, there, here)], axis=0)
    log_decay = jnp.log(1.0 - inflow) + added
    spans = block // REC_SPAN
    rr = lax.broadcasted_iota(jnp.int32, (REC_SPAN, REC_SPAN), 0)
    cc = lax.broadcasted_iota(jnp.int32, (REC_SPAN, REC_SPAN), 1)
    lower = (rr >= cc).astype(F32)
    running, offsets, befores, weighted, grown, shrunk = [], [], [], [], [], []
    for j in (0, 1):
        offset = jnp.zeros((1, w), F32)
        for i in range(spans):
            r = slice(j * block + i * REC_SPAN, j * block + (i + 1) * REC_SPAN)
            run = dot(lower, log_decay[r], precision=lax.Precision.HIGHEST)
            final = run[REC_SPAN - 1 : REC_SPAN]
            running.append(run)
            offsets.append(offset)
            offset = offset + final
            weighted.append((inflow[r] * jnp.exp(final - run)).astype(BF16))
            grown.append(jnp.exp(run))
            shrunk.append((inflow[r] * jnp.exp(-run)).astype(BF16))
        sd[x, j] = jnp.broadcast_to(offset, sd.shape[2:])
    at_end(lambda: on_core(0, lambda: forward(2, 1)))
    at_middle(lambda: forward(2, 2))
    collect(1)
    both = dot(full, jnp.concatenate([weight(at_v), widen(gb[:, at_q:at_r])], axis=1)).astype(BF16)
    vals, queries = both[:, :w], both[:, w:]
    for j in (0, 1):
        carried = None
        for i in range(spans):
            r = slice(j * block + i * REC_SPAN, j * block + (i + 1) * REC_SPAN)
            final = running[j * spans + i][REC_SPAN - 1 : REC_SPAN]
            befores.append(carried)
            new = dot(vals[r], weighted[j * spans + i], TN)
            carried = new if carried is None else carried * jnp.exp(final) + new
        st[x, j] = carried.astype(BF16)
    st_swap(x).start()
    sd_swap(x).start()
    at_end(lambda: on_core(0, last_two))


    def advance(carried, sx, j):
        return carried * jnp.exp(sd[sx, j][0:1]) + st[sx, j].astype(F32)

    def un_pair(z2, owner):
        device = (4 * z2 + 2 * zl + x, t)
        return (
            remote(un.at[owner], un.at[owner], un_send.at[z2], un_recv.at[owner], device),
            remote(ud.at[owner], ud.at[owner], ud_send.at[z2], ud_recv.at[owner], device),
        )

    def un_start(z2):
        for copy in un_pair(z2, zh):
            copy.start()

    def un_wait(owner):
        for copy in un_pair(owner, owner):
            copy.wait_recv()

    def join_units():
        st_swap(1 - x).wait_recv()
        sd_swap(1 - x).wait_recv()
        unit = st[0, 0].astype(F32)
        for sx, j in ((1, 0), (0, 1), (1, 1)):
            unit = advance(unit, sx, j)
        un[zh] = unit.astype(BF16)
        ud[zh] = sd[0, 0] + sd[1, 0] + sd[0, 1] + sd[1, 1]
        loop(zh + 1, count_z, un_start)

    def un_done(z2):
        for copy in un_pair(z2, zh):
            copy.wait_send()

    keyvals.arrive(0)

    zs = max(1, min(count_p, KEY_BLOCK // (2 * block)))
    blocks = count_p // zs
    scale = math.log2(math.e) / math.sqrt(QK_DIM)

    def attend(query, b):
        both = kvb[:, :, pl.ds(b * zs, zs)].reshape(2 * zs * block, kvb.shape[4])
        values = both[:, 2 * QK_DIM :]
        parts = []
        for comp in range(2):
            cols = slice(comp * QK_DIM, (comp + 1) * QK_DIM)
            scores = dot(query[:, cols], both[:, cols], NT)
            peak = jnp.max(scores, axis=1, keepdims=True)
            expo = jnp.exp2((scores - peak) * scale)
            parts += [peak, jnp.sum(expo, axis=1, keepdims=True), dot(expo.astype(BF16), values)]
        return tuple(parts)

    def merge(a, b):
        parts = []
        for comp in range(2):
            pa, ta, wa = a[3 * comp : 3 * comp + 3]
            pc, tc, wc = b[3 * comp : 3 * comp + 3]
            peak = jnp.maximum(pa, pc)
            ea, ec = jnp.exp2((pa - peak) * scale), jnp.exp2((pc - peak) * scale)
            parts += [peak, ta * ea + tc * ec, wa * ea + wc * ec]
        return tuple(parts)

    mine = jnp.where(zl == 0, mapw[:, 0:1], mapw[:, 1:2])
    hidden = []
    for j in (0, 1):
        query = queries[j * block : (j + 1) * block]
        got = attend(query, 0)
        if blocks > 1:
            got = lax.fori_loop(1, blocks, lambda b, g: merge(g, attend(query, b)), got)
        blended = got[2] / got[1] - mine * (got[5] / got[4])
        hidden.append(rms(blended, again[...]))
    attn_hidden = jnp.concatenate(hidden, axis=0).astype(BF16)

    def raw_term(owner):
        rows_in = nf[:, :, :, pl.ds(pl.multiple_of(owner * part, part), part)]
        return dot(rows_in.reshape(2 * block, part), gb[owner, at_r:at_a])

    forward(3, 1)
    stepwise = small and part % 128 == 0
    pieces = (p, sources[1], sources[2], sources[0])
    if stepwise:
        raw = raw_term(2 * pieces[0] + x)
        for q in pieces[1:]:
            raw = raw + raw_term(2 * q + x)
    join_units()
    forward(3, 2)
    if stepwise:
        for q in pieces:
            row_in(q, 2).wait_recv()
            raw = raw + raw_term(2 * q + 1 - x)
    else:
        collect(2)
        raw = dot(full, weight(at_r))
    raw = raw.astype(BF16).astype(F32)
    rec_query = raw * jax.nn.sigmoid(raw)
    local, lifted = [], []
    for j in (0, 1):
        outs, lifts = [], []
        for i in range(spans):
            r = slice(j * block + i * REC_SPAN, j * block + (i + 1) * REC_SPAN)
            m = j * spans + i
            decayed = rec_query[r] * grown[m]
            dq = decayed.astype(BF16)
            within = dot(dq, shrunk[m], NT) * lower
            o = dot(within.astype(BF16), vals[r])
            if befores[m] is not None:
                o = o + dot(dq, befores[m].astype(BF16), NT)
            outs.append(o)
            lifts.append(decayed * jnp.exp(offsets[m]))
        local.append(jnp.concatenate(outs, axis=0))
        lifted.append(jnp.concatenate(lifts, axis=0).astype(BF16))

    forward(3, 0)
    loop(0, zh, un_wait)

    def chain(k, carry):
        return carry * jnp.exp(ud[k][0:1]) + un[k].astype(F32)

    base = lax.fori_loop(0, zh, chain, init[zl].T)
    s01 = advance(base, 0, 0)
    s10 = advance(s01, 1, 0)
    s11 = advance(s10, 0, 1)
    incoming = (jnp.where(x == 0, base, s01), jnp.where(x == 0, s10, s11))
    rec = []
    for j in (0, 1):
        o = local[j] + dot(lifted[j], incoming[j].astype(BF16), NT)
        rec.append(rms(o, rgain[...]))
    rec_hidden = jnp.concatenate(rec, axis=0).astype(BF16)
    both_hidden = jnp.concatenate([rec_hidden, attn_hidden], axis=1)

    per = pb.shape[5] // part
    fw = per * part
    chunks = n // per

    def d_copy(ch):
        return remote(pb.at[ch, 1 - lo], db.at[ch], d_send.at[0], d_recv.at[ch], (s, cmate))

    def y_copy(ch, k, flip):
        h2 = (hi + k) % count_h
        src = zb.at[ch, pl.ds(h2, 1)] if flip else sb.at[ch, pl.ds(2 * h2, 2)]
        dst = yr.at[ch, k, pl.ds(0, 1)] if flip else yr.at[ch, k]
        return remote(src, dst, y_send.at[int(flip)], y_recv.at[ch, k - 1], (s, 2 * h2 + lo))

    def z_copy(ch, flip):
        src = sb.at[ch, pl.ds(count_h * (1 - zl), count_h)] if flip else zb.at[ch, pl.ds(1 - zl, 1)]
        dst = zr.at[ch] if flip else zr.at[ch, pl.ds(0, 1)]
        return remote(src, dst, z_send.at[int(flip)], z_recv.at[ch], (zmate, t))

    def stage_d(ch):
        shard = gb[pl.ds(ch * per, per)]
        weights = jnp.concatenate(
            [shard[:, at_o:].reshape(fw, w), widen(shard[:, at_a:at_o])], axis=1
        )
        got = dot(both_hidden, weights, NT).astype(BF16)
        for z2 in (0, 1):
            for t2 in range(nt):
                lo_row = (z2 * nt + t2) * rows
                pb[ch, t2 % 2, z2, t2 // 2] = got[lo_row : lo_row + rows]
        d_copy(ch).start()

    def stage_first(ch, flip):
        d_copy(ch).wait_recv()
        total = (pb[ch, lo].astype(F32) + db[ch].astype(F32)).astype(BF16)
        if flip:
            sb[ch] = total.reshape(sb.shape[1:])
            z_copy(ch, flip).start()
        else:
            for h2 in range(count_h):
                sb[ch, 2 * h2 : 2 * h2 + 2] = total[:, h2]
            for k in range(1, count_h):
                y_copy(ch, k, flip).start()

    def stage_second(ch, flip):
        if flip:
            z_copy(ch, flip).wait_recv()
            mine = sb[ch, pl.ds(count_h * zl, count_h)]
            zb[ch] = (mine.astype(F32) + zr[ch].astype(F32)).astype(BF16)
            for k in range(1, count_h):
                y_copy(ch, k, flip).start()
        else:
            total = sb[ch, pl.ds(2 * hi, 2)].astype(F32)
            for k in range(1, count_h):
                y_copy(ch, k, flip).wait_recv()
                total = total + yr[ch, k].astype(F32)
            zb[ch, 0:2] = total.astype(BF16)
            z_copy(ch, flip).start()

    def stage_out(ch, flip):
        if flip:
            total = zb[ch, hi].astype(F32)
            for k in range(1, count_h):
                y_copy(ch, k, flip).wait_recv()
                total = total + yr[ch, k, 0].astype(F32)
        else:
            z_copy(ch, flip).wait_recv()
            total = zb[ch, zl].astype(F32) + zr[ch, 0].astype(F32)
        out[:, pl.ds(pl.multiple_of(ch * fw, fw), fw)] = total.astype(out.dtype)
        store(ch).start()

    def store(ch):
        cols = pl.ds(pl.multiple_of(ch * fw, fw), fw)
        return pltpu.make_async_copy(out.at[:, cols], out_ref.at[:, cols], out_sem.at[0])

    if small and per == 1:
        order = [(q, c) for c in (0, 1) for q in (2 * zh, 2 * zh + 1)]
        order += [(q, c) for q in (sources[2], sources[0]) for c in (0, 1)]
        ready = []
        for q, c in order:
            ready.append((2 * q + x if c == 0 else 2 * q + 1 - x, q if c == 1 else None))
    else:
        collect(3)
        ready = [(ch, None) for ch in range(chunks)]

    lag = len(ready)
    for i in range(lag + LAGS[2]):
        if i < lag:
            ch, q = ready[i]
            if q is not None:
                row_in(q, 3).wait_recv()
            stage_d(ch)
        for body, late in zip((stage_first, stage_second, stage_out), LAGS):
            if 0 <= i - late < lag:
                body(ready[i - late][0], (i - late) % 2 == 1)

    sent(gb.at[0 : count_p - 1], col_send.at[0])
    sent(gb.at[0:count_p], row_send.at[0])
    tokens.finish()
    keyvals.finish()
    sent(others, k1_send.at[0])
    kv_swap(x).wait_send()
    extra_swap().wait_send()
    st_swap(x).wait_send()
    sd_swap(x).wait_send()
    loop(zh + 1, count_z, un_done)

    odd = chunks // 2
    even = chunks - odd
    sent(yr.at[0:even, 0 : count_h - 1], y_send.at[0])
    sent(zb.at[0:even, 0:1], z_send.at[0])
    sent(zb.at[0:odd, 0 : count_h - 1], y_send.at[1])
    sent(zb.at[0:odd, 0:count_h], z_send.at[1])
    sent(db, d_send.at[0])
    pltpu.make_async_copy(out, out_ref, out_sem.at[0]).wait()


def solution(mesh):
    n, nt = mesh.shape["sp"], mesh.shape["tp"]

    def body(
        tokens, input_norm_gain, paired_query_weight, shared_key_weight, shared_value_weight,
        recurrent_query_weight, forget_gate_weight, recurrent_value_weight,
        attention_output_weight, recurrent_output_weight, attention_head_gain,
        recurrent_head_gain, second_map_weight, forget_leak_rate, extra_log_decay,
        initial_recurrent_state,
    ):
        rows, width = tokens.shape
        weights = (
            paired_query_weight, forget_gate_weight, recurrent_value_weight,
            recurrent_query_weight, attention_output_weight, recurrent_output_weight,
        )
        part = forget_gate_weight.shape[0]
        span = extra_log_decay.shape[0]
        count_p, count_z, count_h = n // 2, n // 4, nt // 2
        fw = part * max(1, OUT_WIDTH // part)
        chunks = width // fw
        kv_width = 2 * QK_DIM + HEAD_DIM
        wk, wval = shared_key_weight.T, shared_value_weight.T
        staged = (
            tokens, input_norm_gain[None], *weights, wk, wval, attention_head_gain[None],
            recurrent_head_gain[None], second_map_weight[None], forget_leak_rate[None],
            extra_log_decay, initial_recurrent_state,
        )
        hb = pl.BlockSpec(memory_space=pl.ANY)
        dma = pltpu.SemaphoreType.DMA
        w = RECURRENT_WIDTH
        return pl.pallas_call(
            functools.partial(kernel, n, nt),
            out_shape=jax.ShapeDtypeStruct((rows, width), BF16),
            in_specs=[hb] * len(staged),
            out_specs=hb,
            scratch_shapes=[pltpu.VMEM(a.shape, a.dtype) for a in staged] + [
                pltpu.VMEM((rows, width), BF16),
                dma((len(staged),)), dma((1,)),
                pltpu.VMEM((n, 5 * part, w), BF16),
                pltpu.VMEM((5 * part, w), BF16),
                pltpu.VMEM((2, nt, rows, width), BF16),
                pltpu.VMEM((nt, 2, count_p, rows, kv_width), BF16),
                pltpu.VMEM((span, w), BF16),
                pltpu.VMEM((span, w), BF16),
                pltpu.VMEM((2, 2, w, w), BF16),
                pltpu.VMEM((2, 2, 8, w), F32),
                pltpu.VMEM((count_z, w, w), BF16),
                pltpu.VMEM((count_z, 8, w), F32),
                pltpu.VMEM((chunks, 2, 2, count_h, rows, fw), BF16),
                pltpu.VMEM((chunks, 2, count_h, rows, fw), BF16),
                pltpu.VMEM((chunks, 2 * count_h, rows, fw), BF16),
                pltpu.VMEM((chunks, count_h, 2, rows, fw), BF16),
                pltpu.VMEM((chunks, max(2, count_h), rows, fw), BF16),
                pltpu.VMEM((chunks, max(2, count_h), rows, fw), BF16),
                dma((1,)), dma((count_p, 4)),
                dma((1,)), dma((2 + 2 * count_p,)),
                dma((2,)), dma((2 * count_h + 2,)),
                dma((2,)), dma((count_h,)),
                dma((1,)), dma((1,)),
                dma((4,)), dma((4,)),
                dma((count_z,)), dma((count_z,)),
                dma((count_z,)), dma((count_z,)),
                dma((1,)), dma((chunks,)),
                dma((2,)), dma((chunks, count_h - 1)),
                dma((2,)), dma((chunks,)),
            ],
            compiler_params=pltpu.CompilerParams(
                has_side_effects=True, collective_id=0, vmem_limit_bytes=60 * 1024 * 1024
            ),
        )(*staged)

    placed = (
        P(("sp", "tp"), None), P(), P("sp", "tp"), P(), P(), P("sp", "tp"), P("sp", "tp"),
        P("sp", "tp"), P("sp", "tp"), P("sp", "tp"), P(), P(), P("tp"), P("tp"),
        P("sp", "tp"), P("tp", None, None),
    )
    return jax.shard_map(
        body, mesh=mesh, in_specs=placed, out_specs=P(("sp", "tp"), None), check_vma=False
    )
```
